32 devices in a mesh: ep: 4 (over y, x), tp: 8 (over z, core).
Axes of the slice: x: 2, y: 2, z: 4, core: 2. Of those that a mesh axis runs over, the one named last changes fastest.
Arguments:
- tokens: bfloat16 [1024, 2048], P('ep', 'tp'), may hold values from -600 to 600
- pre_gain: float32 [2048], P('tp'), may hold values from 0.1 to 1.9
- expert_gate: bfloat16 [4, 2048, 8192], P('ep', None, 'tp'), may hold values from -0.125 to 0.125
- expert_up: bfloat16 [4, 2048, 8192], P('ep', None, 'tp'), may hold values from -0.125 to 0.125
- expert_down: bfloat16 [4, 8192, 2048], P('ep', 'tp'), may hold values from -8 to 8
- routes: int32 [1024, 2], P('ep'), may hold values from 0 to 3, all different within a row; in each aligned block of 256 rows (0 to 255, 256 to 511, ...) at most 192 rows name the same one
- route_weights: float32 [1024, 2], P('ep'), may hold values from 0.1 to 1
- post_gain: float32 [2048], P('tp'), may hold values from 0.1 to 1.9
Outputs:
- layer_out: bfloat16 [1024, 2048], P('ep', 'tp')
The draws below stay inside these ranges and needn't reach their ends.
Inputs may be any that keep to these rules, and one draw needn't show every extreme that they name: `routes`: each token names 2 different experts. Among the 256 tokens of one index of ep no expert is named more than 192 times, a bound that some expert reaches in some of these blocks.
All inputs are finite; a program needn't handle non-finite values.
Results may differ from the reference program's by a relative error of at most 0.024.
Values may be sent and summed in bfloat16 or wider, within the bound.
A program may use at most 64 MiB of HBM per device.

```python
import math
import jax
import jax.numpy as jnp
import numpy as np
from jax import lax

D = 2048
FF = 8192
TOPK = 2
TOK_EP = 256
EXPERTS = 4
CAP = 192
TOKENS = 1024
N_EP = 4
N_TP = 8


def column_scale(key, count):
    ramp = jnp.arange(count, dtype=jnp.float32) / max(count - 1, 1)
    rough = jax.random.uniform(key, (count,), jnp.float32, -0.35, 0.35)
    return jnp.exp(math.log(10.0) * ramp + rough)


def draw_tokens(key, part):
    keys = jax.random.split(jax.random.fold_in(key, 11), 3)
    entries = jnp.clip(jax.random.normal(keys[0], (TOKENS, D), jnp.float32), -4.0, 4.0)
    row_scale = jnp.exp(jax.random.uniform(keys[1], (TOKENS, 1), jnp.float32, 0.0, math.log(10.0)))
    return (entries * row_scale * column_scale(keys[2], D)[None, :]).astype(jnp.bfloat16)


def draw_expert_down(key, part):
    keys = jax.random.split(jax.random.fold_in(key, 23), 2)
    entries = jnp.clip(jax.random.normal(keys[0], (EXPERTS, FF, D), jnp.float32), -4.0, 4.0)
    scaled = entries * FF ** (-0.5) * column_scale(keys[1], D)[None, None, :]
    return scaled.astype(jnp.bfloat16)


def shard_levels(stream_key, extent, cuts, least, top_value):
    level = 1.0
    for axis_at, shards_of in cuts:
        heights = jax.random.uniform(jax.random.fold_in(jax.random.fold_in(stream_key, 6), axis_at), (shards_of,), jnp.float32, least / len(cuts), top_value / len(cuts))
        level = level * jnp.repeat(jnp.exp(heights), extent[axis_at] // shards_of).reshape((-1,) + (1,) * (len(extent) - 1 - axis_at))
    return level


def shared_out(key, own, number, rows, amount, top, limit, skew):
    ranking = jax.random.permutation(key, amount)
    crowded, usual = shares(amount, rows * top, limit, skew, True), shares(amount, rows * top, limit, skew, False)
    places = jnp.arange(amount)

    def named(lengths, offset_by):
        used = int((lengths > 0).sum())
        fixed = max(1, used // 4)
        shifted = fixed + (places - fixed + offset_by * (used - fixed)) % max(1, amount - fixed)
        return jnp.zeros((amount,), jnp.int32).at[ranking[jnp.where(places < fixed, places, shifted)]].set(jnp.asarray(lengths, jnp.int32))

    lengths = jnp.where(number % 4 == 0, named(crowded, number // 4), named(usual, number - number // 4 - 1))
    mixed = jax.random.permutation(jax.random.fold_in(own, 3), amount)
    source_of, receiver = mixed[0:amount // 2 * 2:2], mixed[1:amount // 2 * 2:2]
    margin = jnp.minimum(lengths[source_of] - 1, limit - lengths[receiver]) // 2
    margin = jnp.where((source_of == ranking[0]) | (receiver == ranking[0]) | (lengths[receiver] == 0), 0, jnp.maximum(margin, 0))
    shifted = jax.random.randint(jax.random.fold_in(own, 4), (amount // 2,), 0, 1 << 20) % (margin + 1)
    lengths = lengths.at[source_of].add(-shifted).at[receiver].add(shifted)
    items = jnp.searchsorted(jnp.cumsum(lengths), jnp.arange(rows * top), side="right").astype(jnp.int32)
    table = items.reshape(top, rows).T
    table = table[jax.random.permutation(jax.random.fold_in(own, 1), rows)]
    offset_by = jax.random.randint(jax.random.fold_in(own, 2), (rows, 1), 0, top)
    return jnp.take_along_axis(table, (jnp.arange(top)[None, :] + offset_by) % top, axis=1)


def shares(amount, total, reach, slope, full):
    weights = [(1 << 20) // math.isqrt(grade ** slope) + 1 for grade in range(1, amount + 1)]
    largest = reach if full else min(reach, max(-(-total // amount), total * weights[0] // sum(weights)))
    least = 1 if total - largest >= amount - 1 else 0
    counts, rest = [largest] + [least] * (amount - 1), total - largest - least * (amount - 1)
    while rest > 0:
        candidates = [i for i in range(1, amount) if counts[i] < largest] or [i for i in range(1, amount) if counts[i] < reach]
        mass, left = sum([weights[i] for i in candidates]), rest
        for i in candidates:
            extra = min(reach - counts[i], max(1, left * weights[i] // mass), rest)
            counts[i] = counts[i] + extra
            rest = rest - extra
    return np.array(counts)


def gaussian(stream_key, dims, spread, most, cuts=(), held_as=jnp.bfloat16):
    values = spread * jax.random.normal(stream_key, dims, jnp.float32)
    if cuts:
        values = values * shard_levels(stream_key, dims, cuts, -0.22, 0.18)
    return jnp.clip(values, -most, most).astype(held_as)


def setup_inputs(seed: int = 0) -> dict:
    key_of = jax.random.split(jax.random.key(seed), 9)
    tokens = draw_tokens(jax.random.fold_in(key_of[8], 71), 0)
    pre_gain = jnp.clip(1.0 + 0.18 * jax.random.normal(key_of[1], (D,), jnp.float32), 0.1, 1.9)
    expert_gate = gaussian(key_of[2], (EXPERTS, D, FF), D ** -0.5, 0.125, ((0, 4), (2, 8)))
    expert_up = gaussian(key_of[3], (EXPERTS, D, FF), D ** -0.5, 0.125, ((0, 4), (2, 8)))
    expert_down = draw_expert_down(jax.random.fold_in(key_of[8], 71), 0)
    routes_keys = jax.random.split(jax.random.fold_in(key_of[5], 1), TOKENS // TOK_EP)
    routes_turns = jax.random.permutation(jax.random.fold_in(key_of[5], 3), TOKENS // TOK_EP)
    routes = jax.vmap(lambda own, number: shared_out(jax.random.fold_in(key_of[5], 2), own, number, TOK_EP, EXPERTS, TOPK, CAP, 2))(routes_keys, routes_turns).reshape((TOKENS, TOPK))
    route_weights = jnp.clip(0.1 + 0.9 * jax.random.uniform(key_of[6], (TOKENS, TOPK), jnp.float32) ** shard_levels(key_of[6], (TOKENS, TOPK), ((0, 4),), -0.2, 0.2), 0.1, 1.0)
    post_gain = jnp.clip(1.0 + 0.18 * jax.random.normal(key_of[7], (D,), jnp.float32), 0.1, 1.9)
    return {"tokens": tokens, "pre_gain": pre_gain, "expert_gate": expert_gate, "expert_up": expert_up, "expert_down": expert_down, "routes": routes, "route_weights": route_weights, "post_gain": post_gain}


EPSILON = 1e-06

def rms_scale(values, gain):
    return values * lax.rsqrt(lax.optimization_barrier(jnp.mean(values * values, axis=-1, keepdims=True)) + EPSILON) * gain.astype(jnp.float32)

def reference(tokens, pre_gain, expert_gate, expert_up, expert_down, routes, route_weights, post_gain):
    normed = rms_scale(tokens.astype(jnp.float32), pre_gain).astype(jnp.bfloat16)
    blocks = routes.reshape(N_EP, TOK_EP, TOPK).astype(jnp.int32)
    onehot = (blocks[..., None] == jnp.arange(EXPERTS, dtype=jnp.int32)).astype(jnp.int32)
    onehot = onehot.reshape(N_EP, TOK_EP * TOPK, EXPERTS)
    earlier = jnp.cumsum(onehot, axis=1) - onehot
    slots = lax.optimization_barrier(jnp.sum(earlier * onehot, axis=-1)).reshape(N_EP, TOK_EP, TOPK).astype(jnp.int32)
    block_ids = jnp.broadcast_to(jnp.arange(N_EP, dtype=jnp.int32)[:, None, None], blocks.shape)
    token_ids = jnp.broadcast_to(block_ids * TOK_EP + jnp.arange(TOK_EP, dtype=jnp.int32)[None, :, None], blocks.shape)
    table = jnp.full((EXPERTS, N_EP, CAP), TOKENS, jnp.int32).at[blocks, block_ids, slots].set(token_ids)
    padded = jnp.concatenate([normed, jnp.zeros((1, D), jnp.bfloat16)], axis=0)
    row_count = N_EP * CAP
    part_units = FF // N_TP

    def one_expert(args):
        row_index, w_gate, w_up, w_down = args
        rows = padded[row_index.reshape(-1)]
        gate_pre = jnp.dot(rows, w_gate, preferred_element_type=jnp.float32)
        up_pre = jnp.dot(rows, w_up, preferred_element_type=jnp.float32)
        hidden = (jax.nn.silu(gate_pre) * up_pre).astype(jnp.bfloat16)
        hidden_blocks = hidden.reshape(row_count, N_TP, part_units).transpose(1, 0, 2)
        weight_blocks = w_down.reshape(N_TP, part_units, D)

        def add_block(running, pair):
            part_hidden, part_weight = pair
            partial_value = jnp.dot(part_hidden, part_weight, preferred_element_type=jnp.float32)
            rounded = lax.optimization_barrier(partial_value.astype(jnp.bfloat16))
            return (running + rounded.astype(jnp.float32), None)
        running, _ = lax.scan(add_block, jnp.zeros((row_count, D), jnp.float32), (hidden_blocks, weight_blocks))
        return running.astype(jnp.bfloat16)
    outputs = lax.map(one_expert, (table, expert_gate, expert_up, expert_down))
    picked = outputs[blocks, block_ids * CAP + slots].reshape(TOKENS, TOPK, D)
    combined = lax.optimization_barrier(jnp.sum(route_weights[:, :, None] * picked.astype(jnp.float32), axis=1))
    return rms_scale(combined, post_gain).astype(jnp.bfloat16)
```

```python
import functools

import jax
import jax.numpy as jnp
from jax import lax
from jax.experimental import pallas as pl
from jax.experimental.pallas import tpu as pltpu
from jax.sharding import PartitionSpec as P

EPSILON = 1e-06


def local(tokens, pre_gain, expert_gate, expert_up, expert_down, routes, route_weights, post_gain):
    local_experts = expert_gate.shape[0]
    groups = lax.axis_size("ep")
    experts_all = local_experts * groups
    tok_rows, part_width = tokens.shape
    full_width = part_width * lax.axis_size("tp")
    capacity = 3 * tok_rows // experts_all
    values = tokens.astype(jnp.float32)
    input_sq = lax.psum(jnp.sum(values * values, axis=-1), "tp")
    normed = (
        values * lax.rsqrt(input_sq / full_width + EPSILON)[:, None] * pre_gain[None, :]
    ).astype(jnp.bfloat16)
    onehot = (routes[:, :, None] == jnp.arange(experts_all, dtype=jnp.int32)).astype(jnp.int32)
    onehot = onehot.reshape(tok_rows * 2, experts_all)
    earlier = jnp.cumsum(onehot, axis=0) - onehot
    slots = jnp.sum(earlier * onehot, axis=-1).reshape(tok_rows, 2)
    positions = routes * capacity + slots
    places = jnp.arange(experts_all * capacity, dtype=jnp.int32)
    first_pick = (places[:, None] == positions[None, :, 0]).astype(jnp.bfloat16)
    second_pick = (places[:, None] == positions[None, :, 1]).astype(jnp.bfloat16)
    dispatch = first_pick + second_pick
    outgoing = jnp.dot(dispatch, normed, preferred_element_type=jnp.float32).astype(jnp.bfloat16)
    arrived = lax.all_to_all(outgoing, "ep", split_axis=0, concat_axis=0, tiled=True)
    fragment = lax.all_gather(arrived, "tp", axis=1, tiled=True)
    count = fragment.shape[1]
    grouped = fragment.reshape(groups, local_experts, capacity, count)
    gate_pre = jnp.einsum(
        "secw,ewf->secf", grouped, expert_gate, preferred_element_type=jnp.float32
    )
    up_pre = jnp.einsum("secw,ewf->secf", grouped, expert_up, preferred_element_type=jnp.float32)
    hidden = (jax.nn.silu(gate_pre) * up_pre).astype(jnp.bfloat16)
    product = jnp.einsum("secf,efd->dsec", hidden, expert_down, preferred_element_type=jnp.float32)
    summed = lax.psum_scatter(
        product.reshape(lax.axis_size("tp") * part_width, groups * local_experts * capacity).astype(
            jnp.bfloat16
        ),
        "tp",
        scatter_dimension=0,
        tiled=True,
    )
    returned = lax.all_to_all(summed, "ep", split_axis=1, concat_axis=1, tiled=True)
    contract = (((0,), (1,)), ((), ()))
    first_out = lax.dot_general(first_pick, returned, contract, preferred_element_type=jnp.float32)
    second_out = lax.dot_general(
        second_pick, returned, contract, preferred_element_type=jnp.float32
    )
    combined = route_weights[:, 0:1] * first_out + route_weights[:, 1:2] * second_out
    output_sq = lax.psum(jnp.sum(combined * combined, axis=-1), "tp")
    scaled = combined * lax.rsqrt(output_sq / full_width + EPSILON)[:, None] * post_gain[None, :]
    return scaled.astype(jnp.bfloat16)


CORES = 2
PIECES = 2
F32 = jnp.float32
BF16 = jnp.bfloat16
MESH = pl.DeviceIdType.MESH


def flip(index, bits):
    place = 1
    while place <= bits:
        if bits & place:
            index = index + place - 2 * place * lax.rem(lax.div(index, place), 2)
        place *= 2
    return index


def flip_traced(index, bits, size):
    total, place = 0, 1
    while place < size:
        total = total + place * lax.rem(lax.div(index, place) + lax.div(bits, place), 2)
        place *= 2
    return total


def fused(
    groups, parts, tok, gain, route, weight, gate_hbm, up_hbm, down_hbm, post, out,
    zbuf, fbuf, gains, route1, weight1, disp, mix, x, xnear, xfar, squares,
    gate, up, down, acc_gate, acc_up, hidden, half, half_in, own, mine, theirs,
    back_near, back_far, csend, cin, zsend, zin, stats,
    wsem, zs, zr, gs, gr, us, ur, rs, rr, ns, nr, bs, br, fs, fr, ds, dr,
    qs, qr, hs, hr, cs, cr, ts, tr, ps, pr,
):
    t, e = lax.axis_index("tp"), lax.axis_index("ep")
    z, c = lax.div(t, CORES), lax.rem(t, CORES)
    levels = parts // CORES
    rows, width = tok.shape
    cap = xnear.shape[1]
    full = parts * width
    e1, e2, e3 = flip(e, 1), flip(e, 2), flip(e, 3)
    first_hop = (1 - c) * e1 + c * e2
    second_hop = (1 - c) * e2 + c * e1

    barrier = pltpu.get_barrier_semaphore()
    for i in range(1, parts):
        pl.semaphore_signal(barrier, inc=1, device_id={"tp": flip(t, i)}, device_id_type=MESH)
    for d in (1, 2):
        pl.semaphore_signal(barrier, inc=1, device_id={"ep": flip(e, d)}, device_id_type=MESH)

    loads = [
        pltpu.make_async_copy(gate_hbm.at[0], gate, wsem.at[0]),
        pltpu.make_async_copy(up_hbm.at[0], up, wsem.at[1]),
        pltpu.make_async_copy(down_hbm.at[0], down, wsem.at[2]),
    ]
    for load in loads:
        load.start()

    def remote(src, dst, send, recv, **device):
        return pltpu.make_async_remote_copy(
            src_ref=src, dst_ref=dst, send_sem=send, recv_sem=recv,
            device_id=device, device_id_type=MESH,
        )

    def piece_of(ref, level, h):
        return ref.at[level, pl.ds(h * (rows // PIECES), rows // PIECES)]

    def token_copy(level, h, up):
        step = 1 if up else -1
        source = piece_of(zbuf, level, h)
        return remote(source, source, zs.at[level, h, int(up)], zr.at[level, h], tp=t + step * CORES)

    def raw_copy(level, h):
        return remote(
            piece_of(zbuf, level, h), piece_of(fbuf, level, h),
            rs.at[level, h], rr.at[level, h], ep=first_hop,
        )

    def relay(k):
        for h in range(PIECES):

            @pl.when(z >= k)
            def _():
                if k:
                    token_copy(z - k, h, True).wait_recv()

                @pl.when(z < levels - 1)
                def _():
                    token_copy(z - k, h, True).start()

            @pl.when(z + k < levels)
            def _():
                if k:
                    token_copy(z + k, h, False).wait_recv()

                @pl.when(z > 0)
                def _():
                    token_copy(z + k, h, False).start()

            raw_copy(flip(z, k), h).start()

    def gain_copy(i, part):
        return remote(gain, gains.at[part], gs.at[i], gr.at[part], tp=flip(t, i))

    def route_copies():
        return (
            remote(route, route1, us.at[0], ur.at[0], ep=first_hop),
            remote(weight, weight1, us.at[1], ur.at[1], ep=first_hop),
        )

    def near_copy(level, source):
        return remote(
            xnear.at[level], x.at[level * CORES + c, source], ns.at[level], nr.at[level],
            ep=second_hop,
        )

    def far_copy(level, source):
        return remote(
            xfar.at[level], x.at[level * CORES + c, source], bs.at[level], br.at[level],
            ep=second_hop,
        )

    def core_copy(level, source, core):
        slot = x.at[level * CORES + core, source]
        return remote(slot, slot, fs.at[level, source], fr.at[level, source], tp=z * CORES + 1 - c)

    def half_copy(level, kind):
        span = pl.ds(groups - 1, 1) if kind else pl.ds(0, groups - 1)
        return remote(
            half.at[level, span], half_in.at[level, span],
            ds.at[level, kind], dr.at[level, kind], tp=z * CORES + 1 - c,
        )

    def back_near_copy(level):
        return remote(
            back_near.at[level], mine.at[level, 1], qs.at[level], qr.at[level], ep=second_hop
        )

    def back_far_copy(level):
        return remote(
            back_far.at[level], theirs.at[level, 1], hs.at[level], hr.at[level], ep=second_hop
        )

    def mixed_copy(level):
        return remote(csend.at[level], cin.at[level], cs.at[level], cr.at[level], ep=first_hop)

    def sum_copy(j):
        bits = 2 if j == 2 else 1
        return remote(
            zsend.at[j], zin.at[j], ts.at[j], tr.at[j], tp=flip(z, bits) * CORES + c
        )

    def stat_copy(i, part):
        return remote(stats.at[t], stats.at[part], ps.at[i], pr.at[part], tp=flip(t, i))

    def plan_rows(which, r, w):
        first, second = r[0:1], r[1:2]
        lanes = lax.broadcasted_iota(jnp.int32, (8, rows), 0)
        names = jnp.where(lanes == 0, e, jnp.where(lanes == 1, second_hop, -1))
        member = jnp.where((names == first) | (names == second), 1.0, 0.0)
        before = jnp.where(
            lax.broadcasted_iota(jnp.int32, (rows, rows), 0)
            < lax.broadcasted_iota(jnp.int32, (rows, rows), 1),
            1.0, 0.0,
        )
        slots = jnp.dot(member.astype(BF16), before.astype(BF16), preferred_element_type=F32)
        slots = jnp.where(member > 0.5, slots, -1.0).astype(jnp.int32)
        lines = lax.broadcasted_iota(jnp.int32, (cap, rows), 0)
        spread = []
        for k, name in enumerate((e, second_hop)):
            hit = lines == slots[k : k + 1]
            disp[which, k * cap : (k + 1) * cap, :] = jnp.where(hit, 1.0, 0.0).astype(BF16)
            chosen = jnp.where(first == name, w[0:1], w[1:2])
            spread.append(jnp.where(hit, chosen, 0.0))
        return spread

    def plan_mix(which, spread):
        for k in range(2):
            mix[which, :, k * cap : (k + 1) * cap] = spread[k].T.astype(BF16)

    acc_gate[...] = jnp.zeros_like(acc_gate)
    acc_up[...] = jnp.zeros_like(acc_up)
    squares[...] = jnp.zeros_like(squares)
    zbuf[z] = tok[...]
    gains[t] = gain[...]
    own_spread = plan_rows(0, route[...], weight[...])

    pl.semaphore_wait(barrier, parts + 1)
    for copy in route_copies():
        copy.start()
    relay(0)

    def pick_own(j):
        level = flip(z, j)
        picked = jnp.dot(disp[0], zbuf[level], preferred_element_type=F32).astype(BF16)
        x[level * CORES + c, e] = picked[:cap]
        core_copy(level, e, c).start()
        xnear[level] = picked[cap:]
        near_copy(level, e).start()

    def pick_far(j):
        level = flip(z, j)
        for h in range(PIECES):
            raw_copy(level, h).wait_recv()
        picked = jnp.dot(disp[1], fbuf[level], preferred_element_type=F32).astype(BF16)
        xfar[level] = picked[cap:]
        far_copy(level, first_hop).start()
        x[level * CORES + c, first_hop] = picked[:cap]
        core_copy(level, first_hop, c).start()

    def pass_far(j):
        level = flip(z, j)
        far_copy(level, e3).wait_recv()
        core_copy(level, e3, c).start()

    def pass_near(j):
        level = flip(z, j)
        near_copy(level, second_hop).wait_recv()
        core_copy(level, second_hop, c).start()

    def piece(part, source):
        values = x[part, source].astype(F32)
        square = values * values
        total = square[:, 0:128]
        for lane in range(128, width, 128):
            total = total + square[:, lane : lane + 128]
        scaled = (values * gains[part]).astype(BF16)
        depth = pl.ds(pl.multiple_of(part * width, 128), width)
        return (
            total,
            jnp.dot(scaled, gate[depth, :], preferred_element_type=F32),
            jnp.dot(scaled, up[depth, :], preferred_element_type=F32),
        )

    def level_sum(level, role):
        source = flip_traced(e, role, groups)
        core_copy(level, source, 1 - c).wait_recv()
        found = (squares[role], acc_gate[role], acc_up[role])
        for core in range(CORES):
            found = [p + q for p, q in zip(piece(level * CORES + core, source), found)]
        return found

    def collect(j, low, high):
        def body(role, carry):
            level = flip_traced(z, j - lax.div(role + 1, 2), levels)
            squares[role], acc_gate[role], acc_up[role] = level_sum(level, role)
            return carry

        lax.fori_loop(low, high, body, 0)

    def activate(low, high):
        def body(role, carry):
            total, gate_part, up_part = level_sum(flip(z, levels - 1), role)
            scale = lax.rsqrt(jnp.sum(total, axis=1, keepdims=True) / full + EPSILON)
            gate_part = gate_part * scale
            share = 0.5 + 0.5 * jnp.tanh(0.5 * gate_part)
            hidden[role] = (gate_part * share * (up_part * scale)).astype(BF16)
            return carry

        lax.fori_loop(low, high, body, 0)

    def descend(j, kind):
        level = flip(z, j)
        span = slice(groups - 1, groups) if kind else slice(0, groups - 1)
        count = 1 if kind else groups - 1
        left = hidden[span].reshape(count * cap, hidden.shape[2])

        def block(core):
            columns = pl.ds(pl.multiple_of((level * CORES + core) * width, 128), width)
            return jnp.dot(left, down[:, columns], preferred_element_type=F32)

        other, this = block(1 - c), block(c)
        half[level, span] = other.reshape(count, cap, width).astype(BF16)
        own[level, span] = this.reshape(count, cap, width)
        half_copy(level, kind).start()

    def summed(level, role):
        return (own[level, role] + half_in[level, role].astype(F32)).astype(BF16)

    def finish_far(j):
        level = flip(z, j)
        half_copy(level, 1).wait_recv()
        back_far[level] = summed(level, groups - 1)
        back_far_copy(level).start()

    def finish_near(j):
        level = flip(z, j)
        half_copy(level, 0).wait_recv()
        back_near[level] = summed(level, 2 - c)
        back_near_copy(level).start()
        theirs[level, 0] = summed(level, 1 + c)
        mine[level, 0] = summed(level, 0)

    def combine(which, results):
        return jnp.dot(
            mix[which], results.reshape(2 * cap, width), preferred_element_type=F32
        )

    def hand_over(j):
        level = flip(z, j)
        back_far_copy(level).wait_recv()
        csend[level] = combine(1, theirs[level]).astype(BF16)
        mixed_copy(level).start()

    def settle(j):
        level = flip(z, j)
        back_near_copy(level).wait_recv()
        combined = combine(0, mine[level])
        mixed_copy(level).wait_recv()
        combined = combined + cin[level].astype(F32)
        for source in {3: (), 2: (3,), 1: (), 0: (2, 1)}[j]:
            sum_copy(source).wait_recv()
            combined = combined + zin[source].astype(F32)
        if j:
            zsend[j] = combined.astype(BF16)
            sum_copy(j).start()
        return combined

    pick_own(0)
    for i in range(1, parts):
        gain_copy(i, t).start()
    for copy in route_copies():
        copy.wait_recv()
    far_spread = plan_rows(1, route1[...], weight1[...])
    plan_mix(0, own_spread)
    plan_mix(1, far_spread)
    for i in range(1, parts):
        gain_copy(i, flip(t, i)).wait_recv()
    loads[0].wait()
    loads[1].wait()
    collect(0, 0, 1)
    for j in range(1, levels):
        relay(j)
        pick_far(j - 1)
        pick_own(j)
        pass_near(j - 1)
        if j > 1:
            pass_far(j - 2)
        collect(j, 1 if j == levels - 1 else 0, 4 if j > 1 else 3)
        if j == levels - 1:
            activate(0, 1)
    pick_far(levels - 1)
    pass_near(levels - 1)
    pass_far(levels - 2)
    collect(levels, 3, 4)
    activate(1, 3)
    pass_far(levels - 1)
    activate(3, 4)
    loads[2].wait()
    descend(3, 1)
    descend(2, 1)
    descend(1, 1)
    finish_far(3)
    descend(0, 1)
    finish_far(2)
    descend(3, 0)
    finish_far(1)
    descend(2, 0)
    finish_far(0)
    finish_near(3)
    descend(1, 0)
    finish_near(2)
    hand_over(3)
    descend(0, 0)
    finish_near(1)
    hand_over(2)
    finish_near(0)
    hand_over(1)
    settle(3)
    hand_over(0)
    for j in range(levels - 2, -1, -1):
        combined = settle(j)

    square = combined * combined
    folded = square[:, 0:128]
    for lane in range(128, width, 128):
        folded = folded + square[:, lane : lane + 128]
    stats[t] = jnp.sum(folded.T.reshape(16, 8, rows), axis=0)
    for i in range(1, parts):
        stat_copy(i, t).start()
    for i in range(1, parts):
        stat_copy(i, flip(t, i)).wait_recv()
    total = jnp.sum(stats[...], axis=0)
    high = total.astype(BF16)
    ones = jnp.ones((8, 128), BF16)
    column = sum(
        lax.dot_general(v, ones, (((0,), (0,)), ((), ())), preferred_element_type=F32)
        for v in (high, (total - high.astype(F32)).astype(BF16))
    )
    scale = lax.rsqrt(column[:, 0:1] / full + EPSILON)
    out[...] = (combined * scale * post[...]).astype(BF16)

    for j in range(levels):

        for h in range(PIECES):

            @pl.when((z >= j) & (z < levels - 1))
            def _():
                token_copy(j, h, True).wait_send()

            @pl.when((z <= j) & (z > 0))
            def _():
                token_copy(j, h, False).wait_send()

            raw_copy(j, h).wait_send()

    for copy in route_copies():
        copy.wait_send()
    for j in range(1, levels):
        sum_copy(j).wait_send()
    for i in range(1, parts):
        gain_copy(i, t).wait_send()
        stat_copy(i, t).wait_send()
    for j in range(levels):
        near_copy(j, e).wait_send()
        far_copy(j, first_hop).wait_send()
        for source in range(groups):
            core_copy(j, source, c).wait_send()
        half_copy(j, 0).wait_send()
        half_copy(j, 1).wait_send()
        back_near_copy(j).wait_send()
        back_far_copy(j).wait_send()
        mixed_copy(j).wait_send()


def local_fused(tokens, pre_gain, expert_gate, expert_up, expert_down, routes, route_weights, post_gain):
    groups, parts = lax.axis_size("ep"), lax.axis_size("tp")
    rows, width = tokens.shape
    _, features, units = expert_gate.shape
    levels = parts // CORES
    cap = 3 * rows // groups
    vmem = pl.BlockSpec(memory_space=pltpu.VMEM)
    anywhere = pl.BlockSpec(memory_space=pl.ANY)
    dma = pltpu.SemaphoreType.DMA
    tok_block = pltpu.VMEM((levels, rows, width), BF16)
    row_block = pltpu.VMEM((levels, cap, width), BF16)
    block = (levels, groups, cap, width)
    return pl.pallas_call(
        functools.partial(fused, groups, parts),
        out_shape=jax.ShapeDtypeStruct((rows, width), BF16),
        in_specs=[vmem] * 4 + [anywhere] * 3 + [vmem],
        out_specs=vmem,
        scratch_shapes=[
            tok_block,
            tok_block,
            pltpu.VMEM((parts, 1, width), F32),
            pltpu.VMEM((2, rows), jnp.int32),
            pltpu.VMEM((2, rows), F32),
            pltpu.VMEM((2, 2 * cap, rows), BF16),
            pltpu.VMEM((2, rows, 2 * cap), BF16),
            pltpu.VMEM((parts, groups, cap, width), BF16),
            row_block,
            row_block,
            pltpu.VMEM((groups, cap, 128), F32),
            pltpu.VMEM((features, units), BF16),
            pltpu.VMEM((features, units), BF16),
            pltpu.VMEM((units, features), BF16),
            pltpu.VMEM((groups, cap, units), F32),
            pltpu.VMEM((groups, cap, units), F32),
            pltpu.VMEM((groups, cap, units), BF16),
            pltpu.VMEM(block, BF16),
            pltpu.VMEM(block, BF16),
            pltpu.VMEM(block, F32),
            pltpu.VMEM((levels, 2, cap, width), BF16),
            pltpu.VMEM((levels, 2, cap, width), BF16),
            row_block,
            row_block,
            tok_block,
            tok_block,
            tok_block,
            tok_block,
            pltpu.VMEM((parts, 8, rows), F32),
            dma((3,)),
            dma((levels, PIECES, 2)), dma((levels, PIECES)),
            dma((parts,)), dma((parts,)),
            dma((2,)), dma((2,)),
            dma((levels, PIECES)), dma((levels, PIECES)),
            dma((levels,)), dma((levels,)),
            dma((levels,)), dma((levels,)),
            dma((levels, groups)), dma((levels, groups)),
            dma((levels, 2)), dma((levels, 2)),
            dma((levels,)), dma((levels,)),
            dma((levels,)), dma((levels,)),
            dma((levels,)), dma((levels,)),
            dma((levels,)), dma((levels,)),
            dma((parts,)), dma((parts,)),
        ],
        compiler_params=pltpu.CompilerParams(
            collective_id=0, has_side_effects=True, vmem_limit_bytes=60 * 1024 * 1024
        ),
    )(
        tokens, pre_gain.reshape(1, width), routes.T, route_weights.T,
        expert_gate, expert_up, expert_down, post_gain.reshape(1, width),
    )


def plan(mesh):
    def choose(*args):
        tokens, gate = args[0], args[2]
        groups, parts = mesh.shape["ep"], mesh.shape["tp"]
        rows, width = tokens.shape
        fits = (
            gate.shape[0] == 1
            and groups == 4
            and parts == 4 * CORES
            and width % 128 == 0
            and rows % 128 == 0
            and (3 * rows // groups) % 64 == 0
            and gate.shape[2] % 128 == 0
        )
        return (local_fused if fits else local)(*args)

    return choose


def solution(mesh):
    placed = (
        P("ep", "tp"),
        P("tp"),
        P("ep", None, "tp"),
        P("ep", None, "tp"),
        P("ep", "tp", None),
        P("ep", None),
        P("ep", None),
        P("tp"),
    )
    return jax.shard_map(
        plan(mesh), mesh=mesh, in_specs=placed, out_specs=P("ep", "tp"), check_vma=False
    )
```

```python
import functools

import jax
import jax.numpy as jnp
from jax import lax
from jax.experimental import pallas as pl
from jax.experimental.pallas import tpu as pltpu
from jax.sharding import PartitionSpec as P

EPSILON = 1e-06


def local(tokens, pre_gain, expert_gate, expert_up, expert_down, routes, route_weights, post_gain):
    local_experts = expert_gate.shape[0]
    groups = lax.axis_size("ep")
    experts_all = local_experts * groups
    tok_rows, part_width = tokens.shape
    full_width = part_width * lax.axis_size("tp")
    capacity = 3 * tok_rows // experts_all
    values = tokens.astype(jnp.float32)
    input_sq = lax.psum(jnp.sum(values * values, axis=-1), "tp")
    normed = (
        values * lax.rsqrt(input_sq / full_width + EPSILON)[:, None] * pre_gain[None, :]
    ).astype(jnp.bfloat16)
    onehot = (routes[:, :, None] == jnp.arange(experts_all, dtype=jnp.int32)).astype(jnp.int32)
    onehot = onehot.reshape(tok_rows * 2, experts_all)
    earlier = jnp.cumsum(onehot, axis=0) - onehot
    slots = jnp.sum(earlier * onehot, axis=-1).reshape(tok_rows, 2)
    positions = routes * capacity + slots
    places = jnp.arange(experts_all * capacity, dtype=jnp.int32)
    first_pick = (places[:, None] == positions[None, :, 0]).astype(jnp.bfloat16)
    second_pick = (places[:, None] == positions[None, :, 1]).astype(jnp.bfloat16)
    dispatch = first_pick + second_pick
    outgoing = jnp.dot(dispatch, normed, preferred_element_type=jnp.float32).astype(jnp.bfloat16)
    arrived = lax.all_to_all(outgoing, "ep", split_axis=0, concat_axis=0, tiled=True)
    fragment = lax.all_gather(arrived, "tp", axis=1, tiled=True)
    count = fragment.shape[1]
    grouped = fragment.reshape(groups, local_experts, capacity, count)
    gate_pre = jnp.einsum(
        "secw,ewf->secf", grouped, expert_gate, preferred_element_type=jnp.float32
    )
    up_pre = jnp.einsum("secw,ewf->secf", grouped, expert_up, preferred_element_type=jnp.float32)
    hidden = (jax.nn.silu(gate_pre) * up_pre).astype(jnp.bfloat16)
    product = jnp.einsum("secf,efd->dsec", hidden, expert_down, preferred_element_type=jnp.float32)
    summed = lax.psum_scatter(
        product.reshape(lax.axis_size("tp") * part_width, groups * local_experts * capacity).astype(
            jnp.bfloat16
        ),
        "tp",
        scatter_dimension=0,
        tiled=True,
    )
    returned = lax.all_to_all(summed, "ep", split_axis=1, concat_axis=1, tiled=True)
    contract = (((0,), (1,)), ((), ()))
    first_out = lax.dot_general(first_pick, returned, contract, preferred_element_type=jnp.float32)
    second_out = lax.dot_general(
        second_pick, returned, contract, preferred_element_type=jnp.float32
    )
    combined = route_weights[:, 0:1] * first_out + route_weights[:, 1:2] * second_out
    output_sq = lax.psum(jnp.sum(combined * combined, axis=-1), "tp")
    scaled = combined * lax.rsqrt(output_sq / full_width + EPSILON)[:, None] * post_gain[None, :]
    return scaled.astype(jnp.bfloat16)


CORES = 2
PIECES = 4
HALVES = 2
F32 = jnp.float32
BF16 = jnp.bfloat16
MESH = pl.DeviceIdType.MESH


def flip(index, bits):
    place = 1
    while place <= bits:
        if bits & place:
            index = index + place - 2 * place * lax.rem(lax.div(index, place), 2)
        place *= 2
    return index


BATCHES = (
    ((0, 0),), ((0, 1),), ((1, 0), (2, 0)), ((3, 0), (0, 2)), ((1, 1), (2, 1)), ((3, 1), (0, 3)),
    ((1, 2), (2, 2)), ((3, 2),), ((1, 3),), ((2, 3),), ((3, 3),),
)


def fused(
    groups, parts, tok, gain, route_in, weight_in, gate_hbm, up_hbm, down_hbm, post_in, out,
    zbuf, gains, route, weight, post, disp, mix, x, xsend, squares,
    gate, up, down, acc_gate, acc_up, hidden, half, half_in, own, back, ret,
    hand, hand_in, zsend, zin, stats,
    isem, wsem, zs, zr, gs, gr, ns, nr, fs, fr, ds, dr, qs, qr, hs, hr, ts, tr, ps, pr,
):
    t, e = lax.axis_index("tp"), lax.axis_index("ep")
    z, c = lax.div(t, CORES), lax.rem(t, CORES)
    levels = parts // CORES
    rows, width = zbuf.shape[1:]
    cap = xsend.shape[2]
    full = parts * width
    around = [flip(e, role) if role else e for role in range(groups)]
    batch_of = {unit: k for k, batch in enumerate(BATCHES) for unit in batch}

    barrier = pltpu.get_barrier_semaphore()
    for i in range(1, parts):
        pl.semaphore_signal(barrier, inc=1, device_id={"tp": flip(t, i)}, device_id_type=MESH)
    for d in range(1, groups):
        pl.semaphore_signal(barrier, inc=1, device_id={"ep": flip(e, d)}, device_id_type=MESH)

    inputs = [
        pltpu.make_async_copy(route_in, route, isem.at[0]),
        pltpu.make_async_copy(weight_in, weight, isem.at[1]),
        pltpu.make_async_copy(tok, zbuf.at[z], isem.at[2]),
        pltpu.make_async_copy(gain, gains.at[t], isem.at[3]),
        pltpu.make_async_copy(post_in, post, isem.at[4]),
    ]
    for copy in inputs:
        copy.start()
    loads = [
        pltpu.make_async_copy(gate_hbm.at[0], gate, wsem.at[0]),
        pltpu.make_async_copy(up_hbm.at[0], up, wsem.at[1]),
        pltpu.make_async_copy(down_hbm.at[0], down, wsem.at[2]),
    ]
    for load in loads:
        load.start()

    def remote(src, dst, send, recv, **device):
        return pltpu.make_async_remote_copy(
            src_ref=src, dst_ref=dst, send_sem=send, recv_sem=recv,
            device_id=device, device_id_type=MESH,
        )

    def piece_of(ref, level, h, count):
        return ref.at[level, pl.ds(h * (rows // count), rows // count)]

    def token_copy(level, h, up):
        step = 1 if up else -1
        source = piece_of(zbuf, level, h, PIECES)
        return remote(source, source, zs.at[int(up)], zr.at[level, h], tp=t + step * CORES)

    def relay(k, h):
        @pl.when(z >= k)
        def _():
            if k:
                token_copy(z - k, h, True).wait_recv()

            @pl.when(z < levels - 1)
            def _():
                token_copy(z - k, h, True).start()

        @pl.when(z + k < levels)
        def _():
            if k:
                token_copy(z + k, h, False).wait_recv()

            @pl.when(z > 0)
            def _():
                token_copy(z + k, h, False).start()

    def gain_copy(i, part):
        return remote(gains.at[part], gains.at[part], gs, gr, tp=flip(t, i))

    def row_copy(level, role, source):
        return remote(
            xsend.at[level, role - 1], x.at[level * CORES + c, source],
            ns, nr.at[level, role - 1], ep=around[role],
        )

    def core_copy(j, role):
        slot = x.at[flip(z, j) * CORES + c, around[role]]
        return remote(slot, slot, fs, fr.at[batch_of[role, j]], tp=z * CORES + 1 - c)

    def half_copy(level, kind):
        span = pl.ds(groups - 1, 1) if kind else pl.ds(0, groups - 1)
        return remote(
            half.at[level, span], half_in.at[level, span],
            ds, dr.at[level, kind], tp=z * CORES + 1 - c,
        )

    def back_copy(level, role):
        return remote(
            back.at[level, role - 1], ret.at[level, role],
            qs, qr.at[level, role - 1], ep=around[role],
        )

    def hand_copy(kind):
        span = pl.ds(groups - 1, 1) if kind else pl.ds(0, groups - 1)
        return remote(
            hand.at[span], hand_in.at[span], hs, hr.at[kind], tp=flip(z, 1) * CORES + c
        )

    def sum_copy(j, h):
        bits = 2 if j == 2 else 1
        return remote(
            piece_of(zsend, j, h, HALVES), piece_of(zin, j, h, HALVES),
            ts, tr.at[j, h], tp=flip(z, bits) * CORES + c,
        )

    def stat_copy(i, part):
        return remote(stats.at[t], stats.at[part], ps, pr, tp=flip(t, i))

    def plan_rows():
        r, w = route[...], weight[...]
        first, second = r[0:1], r[1:2]
        lanes = lax.broadcasted_iota(jnp.int32, (8, rows), 0)
        names = jnp.full((8, rows), -1, jnp.int32)
        for role in range(groups):
            names = jnp.where(lanes == role, around[role], names)
        member = jnp.where((names == first) | (names == second), 1.0, 0.0)
        before = jnp.where(
            lax.broadcasted_iota(jnp.int32, (rows, rows), 0)
            < lax.broadcasted_iota(jnp.int32, (rows, rows), 1),
            1.0, 0.0,
        )
        slots = jnp.dot(member.astype(BF16), before.astype(BF16), preferred_element_type=F32)
        slots = jnp.where(member > 0.5, slots, -1.0).astype(jnp.int32)
        lines = lax.broadcasted_iota(jnp.int32, (cap, rows), 0)
        spread = []
        for role in range(groups):
            hit = lines == slots[role : role + 1]
            disp[role * cap : (role + 1) * cap, :] = jnp.where(hit, 1.0, 0.0).astype(BF16)
            chosen = jnp.where(first == around[role], w[0:1], w[1:2])
            spread.append(jnp.where(hit, chosen, 0.0))
        return spread

    def plan_mix(spread):
        mix[...] = jnp.concatenate(spread, axis=0).T.astype(BF16)

    for copy in inputs[:4]:
        copy.wait()
    pl.semaphore_wait(barrier, parts + groups - 2)
    for i in range(1, parts):
        gain_copy(i, t).start()
    for h in range(PIECES):
        relay(0, h)

    def pick(j):
        level = flip(z, j)
        picked = jnp.dot(disp[...], zbuf[level], preferred_element_type=F32).astype(BF16)
        for role in range(1, groups):
            xsend[level, role - 1] = picked[role * cap : (role + 1) * cap]
        x[level * CORES + c, e] = picked[:cap]
        for role in range(1, groups):
            row_copy(level, role, e).start()
        core_copy(j, 0).start()

    def pass_on(j, role):
        row_copy(flip(z, j), role, around[role]).wait_recv()
        core_copy(j, role).start()

    def level_sum(j, role):
        level, source = flip(z, j), around[role]
        total, scaled = 0.0, []
        for core in range(CORES):
            part = level * CORES + core
            values = x[part, source].astype(F32)
            square = values * values
            for lane in range(0, width, 128):
                total = total + square[:, lane : lane + 128]
            scaled.append((values * gains[part]).astype(BF16))
        left = jnp.concatenate(scaled, axis=1)
        depth = pl.ds(pl.multiple_of(level * CORES * width, CORES * 128), CORES * width)
        found = (
            total,
            jnp.dot(left, gate[depth, :], preferred_element_type=F32),
            jnp.dot(left, up[depth, :], preferred_element_type=F32),
        )
        if j:
            found = [p + ref[role] for p, ref in zip(found, (squares, acc_gate, acc_up))]
        return found

    def project(k):
        batch = BATCHES[k]
        slots = x.at[0, pl.ds(0, len(batch))]
        remote(slots, slots, fs, fr.at[k], tp=z * CORES + 1 - c).wait_recv()
        for role, j in batch:
            found = level_sum(j, role)
            if j < levels - 1:
                squares[role], acc_gate[role], acc_up[role] = found
                continue
            total, gate_part, up_part = found
            scale = lax.rsqrt(jnp.sum(total, axis=1, keepdims=True) / full + EPSILON)
            gate_part = gate_part * scale
            share = 0.5 + 0.5 * jnp.tanh(0.5 * gate_part)
            hidden[role] = (gate_part * share * (up_part * scale)).astype(BF16)

    def descend(j, kind):
        level = flip(z, j)
        span = slice(groups - 1, groups) if kind else slice(0, groups - 1)
        count = 1 if kind else groups - 1
        left = hidden[span].reshape(count * cap, hidden.shape[2])

        def block(core):
            columns = pl.ds(pl.multiple_of((level * CORES + core) * width, 128), width)
            return jnp.dot(left, down[:, columns], preferred_element_type=F32)

        other, this = block(1 - c), block(c)
        half[level, span] = other.reshape(count, cap, width).astype(BF16)
        own[level, span] = this.reshape(count, cap, width)
        half_copy(level, kind).start()

    def finish(j, kind):
        level = flip(z, j)
        half_copy(level, kind).wait_recv()
        if j == 0:
            hand_copy(kind).wait_recv()
        for role in (groups - 1,) if kind else range(1, groups):
            role = role if kind else role % (groups - 1)
            found = own[level, role] + half_in[level, role].astype(F32)
            if j == 0:
                found = found + hand_in[role].astype(F32)
            if j == 1:
                hand[role] = found.astype(BF16)
            elif role:
                back[level, role - 1] = found.astype(BF16)
                back_copy(level, role).start()
            else:
                ret[level, 0] = found.astype(BF16)
        if j == 1:
            hand_copy(kind).start()

    def settle(j):
        level = flip(z, j)
        for role in range(groups - 1, 0, -1):
            back_copy(level, role).wait_recv()
        combined = jnp.dot(
            mix[...], ret[level].reshape(groups * cap, width), preferred_element_type=F32
        )
        found = []
        for h in range(HALVES):
            part = combined[h * (rows // HALVES) : (h + 1) * (rows // HALVES)]
            for source in {3: (), 2: (3,), 0: (2,)}[j]:
                sum_copy(source, h).wait_recv()
                arrived = zin[source, h * (rows // HALVES) : (h + 1) * (rows // HALVES)]
                part = part + arrived.astype(F32)
            if j:
                zsend[j, h * (rows // HALVES) : (h + 1) * (rows // HALVES)] = part.astype(BF16)
                sum_copy(j, h).start()
            found.append(part)
        return jnp.concatenate(found, axis=0)

    spread = plan_rows()
    pick(0)
    plan_mix(spread)
    spare = gains.at[pl.ds(0, parts - 1)]
    remote(spare, spare, gs, gr, tp=flip(t, 1)).wait_recv()
    inputs[4].wait()
    loads[0].wait()
    loads[1].wait()
    project(0)
    for h in range(PIECES):
        relay(1, h)
    pick(1)
    pass_on(0, 1)
    pass_on(0, 2)
    relay(2, 0)
    project(1)
    relay(2, 1)
    project(2)
    relay(2, 2)
    relay(2, 3)
    pick(2)
    pass_on(0, 3)
    relay(3, 0)
    relay(3, 1)
    project(3)
    relay(3, 2)
    relay(3, 3)
    pick(3)
    pass_on(1, 1)
    pass_on(1, 2)
    pass_on(1, 3)
    project(4)
    project(5)
    pass_on(2, 1)
    pass_on(2, 2)
    pass_on(2, 3)
    project(6)
    project(7)
    pass_on(3, 1)
    pass_on(3, 2)
    project(8)
    project(9)
    pass_on(3, 3)
    loads[2].wait()
    descend(3, 0)
    descend(1, 0)
    project(10)
    finish(3, 0)
    finish(1, 0)
    descend(3, 1)
    descend(1, 1)
    descend(2, 0)
    finish(3, 1)
    descend(2, 1)
    finish(2, 0)
    finish(2, 1)
    descend(0, 0)
    descend(0, 1)
    settle(3)
    finish(1, 1)
    finish(0, 0)
    settle(2)
    finish(0, 1)
    combined = settle(0)

    square = combined * combined
    folded = square[:, 0:128]
    for lane in range(128, width, 128):
        folded = folded + square[:, lane : lane + 128]
    stats[t] = jnp.sum(folded.T, axis=0, keepdims=True)
    for i in range(1, parts):
        stat_copy(i, t).start()
    def sent(ref, sem):
        remote(ref, ref, sem, sem, tp=flip(t, 1)).wait_send()

    for k in range(levels):

        @pl.when((z == k) & (z < levels - 1))
        def _():
            sent(zbuf.at[pl.ds(0, k + 1)], zs.at[1])

        @pl.when((z == k) & (z > 0))
        def _():
            sent(zbuf.at[pl.ds(0, levels - k)], zs.at[0])

    for ref, sem in (
        (xsend, ns), (x.at[pl.ds(0, levels)], fs), (half, ds), (hand, hs),
        (back.at[pl.ds(1, levels - 1)], qs), (zsend.at[pl.ds(2, levels - 2)], ts), (spare, gs),
    ):
        sent(ref, sem)
    seen = stats.at[pl.ds(0, parts - 1)]
    remote(seen, seen, ps, pr, tp=flip(t, 1)).wait_recv()
    total = jnp.sum(stats[...], axis=0)
    high = total.astype(BF16)
    ones = jnp.ones((1, 128), BF16)
    column = sum(
        lax.dot_general(v, ones, (((0,), (0,)), ((), ())), preferred_element_type=F32)
        for v in (high, (total - high.astype(F32)).astype(BF16))
    )
    scale = lax.rsqrt(column[:, 0:1] / full + EPSILON)
    out[...] = (combined * scale * post[...]).astype(BF16)
    sent(seen, ps)


def local_fused(tokens, pre_gain, expert_gate, expert_up, expert_down, routes, route_weights, post_gain):
    groups, parts = lax.axis_size("ep"), lax.axis_size("tp")
    rows, width = tokens.shape
    _, features, units = expert_gate.shape
    levels = parts // CORES
    cap = 3 * rows // groups
    vmem = pl.BlockSpec(memory_space=pltpu.VMEM)
    anywhere = pl.BlockSpec(memory_space=pl.ANY)
    dma = pltpu.SemaphoreType.DMA
    tok_block = pltpu.VMEM((levels, rows, width), BF16)
    block = (levels, groups, cap, width)
    away = pltpu.VMEM((levels, groups - 1, cap, width), BF16)
    return pl.pallas_call(
        functools.partial(fused, groups, parts),
        out_shape=pltpu.VMEM((rows, width), BF16),
        in_specs=[anywhere] * 8,
        out_specs=vmem,
        scratch_shapes=[
            tok_block,
            pltpu.VMEM((parts, 1, width), F32),
            pltpu.VMEM((2, rows), jnp.int32),
            pltpu.VMEM((2, rows), F32),
            pltpu.VMEM((1, width), F32),
            pltpu.VMEM((groups * cap, rows), BF16),
            pltpu.VMEM((rows, groups * cap), BF16),
            pltpu.VMEM((parts, groups, cap, width), BF16),
            away,
            pltpu.VMEM((groups, cap, 128), F32),
            pltpu.VMEM((features, units), BF16),
            pltpu.VMEM((features, units), BF16),
            pltpu.VMEM((units, features), BF16),
            pltpu.VMEM((groups, cap, units), F32),
            pltpu.VMEM((groups, cap, units), F32),
            pltpu.VMEM((groups, cap, units), BF16),
            pltpu.VMEM(block, BF16),
            pltpu.VMEM(block, BF16),
            pltpu.VMEM(block, F32),
            away,
            pltpu.VMEM(block, BF16),
            pltpu.VMEM((groups, cap, width), BF16),
            pltpu.VMEM((groups, cap, width), BF16),
            tok_block,
            tok_block,
            pltpu.VMEM((parts, 1, rows), F32),
            dma((5,)), dma((3,)),
            dma((2,)), dma((levels, PIECES)),
            dma, dma,
            dma, dma((levels, groups - 1)),
            dma, dma((len(BATCHES),)),
            dma, dma((levels, 2)),
            dma, dma((levels, groups - 1)),
            dma, dma((2,)),
            dma, dma((levels, HALVES)),
            dma, dma,
        ],
        compiler_params=pltpu.CompilerParams(
            collective_id=0, has_side_effects=True, vmem_limit_bytes=60 * 1024 * 1024
        ),
    )(
        tokens, pre_gain.reshape(1, width), routes.T, route_weights.T,
        expert_gate, expert_up, expert_down, post_gain.reshape(1, width),
    )


def plan(mesh):
    def choose(*args):
        tokens, gate = args[0], args[2]
        groups, parts = mesh.shape["ep"], mesh.shape["tp"]
        rows, width = tokens.shape
        fits = (
            gate.shape[0] == 1
            and groups == 4
            and parts == 4 * CORES
            and width % 128 == 0
            and rows % 128 == 0
            and (3 * rows // groups) % 64 == 0
            and gate.shape[2] % 128 == 0
        )
        return (local_fused if fits else local)(*args)

    return choose


def solution(mesh):
    placed = (
        P("ep", "tp"),
        P("tp"),
        P("ep", None, "tp"),
        P("ep", None, "tp"),
        P("ep", "tp", None),
        P("ep", None),
        P("ep", None),
        P("tp"),
    )
    return jax.shard_map(
        plan(mesh), mesh=mesh, in_specs=placed, out_specs=P("ep", "tp"), check_vma=False
    )
```

```python
import functools

import jax
import jax.numpy as jnp
from jax import lax
from jax.experimental import pallas as pl
from jax.experimental.pallas import tpu as pltpu
from jax.sharding import PartitionSpec as P

EPSILON = 1e-06


def local(tokens, pre_gain, expert_gate, expert_up, expert_down, routes, route_weights, post_gain):
    local_experts = expert_gate.shape[0]
    groups = lax.axis_size("ep")
    experts_all = local_experts * groups
    tok_rows, part_width = tokens.shape
    full_width = part_width * lax.axis_size("tp")
    capacity = 3 * tok_rows // experts_all
    values = tokens.astype(jnp.float32)
    input_sq = lax.psum(jnp.sum(values * values, axis=-1), "tp")
    normed = (
        values * lax.rsqrt(input_sq / full_width + EPSILON)[:, None] * pre_gain[None, :]
    ).astype(jnp.bfloat16)
    onehot = (routes[:, :, None] == jnp.arange(experts_all, dtype=jnp.int32)).astype(jnp.int32)
    onehot = onehot.reshape(tok_rows * 2, experts_all)
    earlier = jnp.cumsum(onehot, axis=0) - onehot
    slots = jnp.sum(earlier * onehot, axis=-1).reshape(tok_rows, 2)
    positions = routes * capacity + slots
    places = jnp.arange(experts_all * capacity, dtype=jnp.int32)
    first_pick = (places[:, None] == positions[None, :, 0]).astype(jnp.bfloat16)
    second_pick = (places[:, None] == positions[None, :, 1]).astype(jnp.bfloat16)
    dispatch = first_pick + second_pick
    outgoing = jnp.dot(dispatch, normed, preferred_element_type=jnp.float32).astype(jnp.bfloat16)
    arrived = lax.all_to_all(outgoing, "ep", split_axis=0, concat_axis=0, tiled=True)
    fragment = lax.all_gather(arrived, "tp", axis=1, tiled=True)
    count = fragment.shape[1]
    grouped = fragment.reshape(groups, local_experts, capacity, count)
    gate_pre = jnp.einsum(
        "secw,ewf->secf", grouped, expert_gate, preferred_element_type=jnp.float32
    )
    up_pre = jnp.einsum("secw,ewf->secf", grouped, expert_up, preferred_element_type=jnp.float32)
    hidden = (jax.nn.silu(gate_pre) * up_pre).astype(jnp.bfloat16)
    product = jnp.einsum("secf,efd->dsec", hidden, expert_down, preferred_element_type=jnp.float32)
    summed = lax.psum_scatter(
        product.reshape(lax.axis_size("tp") * part_width, groups * local_experts * capacity).astype(
            jnp.bfloat16
        ),
        "tp",
        scatter_dimension=0,
        tiled=True,
    )
    returned = lax.all_to_all(summed, "ep", split_axis=1, concat_axis=1, tiled=True)
    contract = (((0,), (1,)), ((), ()))
    first_out = lax.dot_general(first_pick, returned, contract, preferred_element_type=jnp.float32)
    second_out = lax.dot_general(
        second_pick, returned, contract, preferred_element_type=jnp.float32
    )
    combined = route_weights[:, 0:1] * first_out + route_weights[:, 1:2] * second_out
    output_sq = lax.psum(jnp.sum(combined * combined, axis=-1), "tp")
    scaled = combined * lax.rsqrt(output_sq / full_width + EPSILON)[:, None] * post_gain[None, :]
    return scaled.astype(jnp.bfloat16)


CORES = 2
PIECES = 4
HALVES = 4
F32 = jnp.float32
BF16 = jnp.bfloat16
MESH = pl.DeviceIdType.MESH


def flip(index, bits):
    place = 1
    while place <= bits:
        if bits & place:
            index = index + place - 2 * place * lax.rem(lax.div(index, place), 2)
        place *= 2
    return index


BATCHES = (
    ((0, 0), (0, 1)), ((1, 0), (2, 0)), ((3, 0), (0, 2)), ((1, 1), (2, 1)), ((0, 3),),
    ((1, 2), (2, 2)), ((3, 1), (3, 2)), ((1, 3),), ((2, 3),), ((3, 3),),
)


def fused(
    groups, parts, tok, gain, route_in, weight_in, gate_hbm, up_hbm, down_hbm, post_in, out,
    zbuf, gains, route, weight, post, disp, mix, x, xsend, squares,
    gate, up, down, acc_gate, acc_up, hidden, half, half_in, own, back, ret,
    hand, hand_in, zsend, zin, stats,
    isem, wsem, zs, zr, gs, gr, ns, nr, ks, kr, fs, fr, ds, dr, qs, qr, hs, hr, ts, tr, ps, pr,
):
    t, e = lax.axis_index("tp"), lax.axis_index("ep")
    z, c = lax.div(t, CORES), lax.rem(t, CORES)
    levels = parts // CORES
    rows, width = zbuf.shape[1:]
    cap = xsend.shape[1]
    full = parts * width
    around = [flip(e, role) if role else e for role in range(groups)]
    batch_of = {unit: k for k, batch in enumerate(BATCHES) for unit in batch}

    barrier = pltpu.get_barrier_semaphore()
    for i in range(1, parts):
        pl.semaphore_signal(barrier, inc=1, device_id={"tp": flip(t, i)}, device_id_type=MESH)
    for d in range(1, groups):
        pl.semaphore_signal(barrier, inc=1, device_id={"ep": flip(e, d)}, device_id_type=MESH)

    inputs = [
        pltpu.make_async_copy(route_in, route, isem.at[0]),
        pltpu.make_async_copy(weight_in, weight, isem.at[1]),
        pltpu.make_async_copy(tok, zbuf.at[z], isem.at[2]),
        pltpu.make_async_copy(gain, gains.at[t], isem.at[3]),
        pltpu.make_async_copy(post_in, post, isem.at[4]),
    ]
    for copy in inputs:
        copy.start()
    loads = [
        pltpu.make_async_copy(gate_hbm.at[0], gate, wsem.at[0]),
        pltpu.make_async_copy(up_hbm.at[0], up, wsem.at[1]),
        pltpu.make_async_copy(down_hbm.at[0], down, wsem.at[2]),
    ]
    for load in loads:
        load.start()

    def remote(src, dst, send, recv, **device):
        return pltpu.make_async_remote_copy(
            src_ref=src, dst_ref=dst, send_sem=send, recv_sem=recv,
            device_id=device, device_id_type=MESH,
        )

    def piece_of(ref, level, h, count):
        return ref.at[level, pl.ds(h * (rows // count), rows // count)]

    def token_copy(level, h, up):
        step = 1 if up else -1
        source = piece_of(zbuf, level, h, PIECES)
        return remote(source, source, zs.at[int(up)], zr.at[level, h], tp=t + step * CORES)

    def relay(k, h):
        @pl.when(z >= k)
        def _():
            if k:
                token_copy(z - k, h, True).wait_recv()

            @pl.when(z < levels - 1)
            def _():
                token_copy(z - k, h, True).start()

        @pl.when(z + k < levels)
        def _():
            if k:
                token_copy(z + k, h, False).wait_recv()

            @pl.when(z > 0)
            def _():
                token_copy(z + k, h, False).start()

    def gain_copy(i, part):
        return remote(gains.at[part], gains.at[part], gs, gr, tp=flip(t, i))

    def row_copy(level, role, source):
        return remote(
            xsend.at[level * (groups - 1) + role - 1], x.at[level * CORES + c, source],
            ns, nr.at[level, role - 1], ep=around[role],
        )

    def core_copy(j, role):
        slot = x.at[flip(z, j) * CORES + c, around[role]]
        return remote(slot, slot, fs, fr.at[batch_of[role, j]], tp=z * CORES + 1 - c)

    def half_copy(level, kind):
        span = pl.ds(groups - 1, 1) if kind else pl.ds(0, groups - 1)
        return remote(
            half.at[level, span], half_in.at[level, span],
            ds, dr.at[level, kind], tp=z * CORES + 1 - c,
        )

    def back_copy(level, role):
        return remote(
            back.at[level, role - 1], ret.at[level, role],
            qs, qr.at[level, role - 1], ep=around[role],
        )

    def hand_copy(k):
        span = (pl.ds(1, groups - 2), pl.ds(groups - 1, 1), pl.ds(0, 1))[k]
        return remote(
            hand.at[span], hand_in.at[span], hs, hr.at[k], tp=flip(z, 1) * CORES + c
        )

    def sum_copy(j, h):
        bits = 2 if j == 2 else 1
        return remote(
            piece_of(zsend, j, h, HALVES), piece_of(zin, j, h, HALVES),
            ts, tr.at[j - 2, h], tp=flip(z, bits) * CORES + c,
        )

    def stat_copy(i, part):
        return remote(stats.at[t], stats.at[part], ps, pr, tp=flip(t, i))

    def plan_rows():
        r, w = route[...], weight[...]
        first, second = r[0:1], r[1:2]
        lanes = lax.broadcasted_iota(jnp.int32, (8, rows), 0)
        names = jnp.full((8, rows), -1, jnp.int32)
        for role in range(groups):
            names = jnp.where(lanes == role, around[role], names)
        member = jnp.where((names == first) | (names == second), 1.0, 0.0)
        before = jnp.where(
            lax.broadcasted_iota(jnp.int32, (rows, rows), 0)
            < lax.broadcasted_iota(jnp.int32, (rows, rows), 1),
            1.0, 0.0,
        )
        slots = jnp.dot(member.astype(BF16), before.astype(BF16), preferred_element_type=F32)
        slots = jnp.where(member > 0.5, slots, -1.0).astype(jnp.int32)
        lines = lax.broadcasted_iota(jnp.int32, (cap, rows), 0)
        spread = []
        for role in range(groups):
            hit = lines == slots[role : role + 1]
            disp[role * cap : (role + 1) * cap, :] = jnp.where(hit, 1.0, 0.0).astype(BF16)
            chosen = jnp.where(first == around[role], w[0:1], w[1:2])
            spread.append(jnp.where(hit, chosen, 0.0))
        return spread

    def plan_mix(spread):
        mix[...] = jnp.concatenate(spread, axis=0).T.astype(BF16)

    for copy in inputs[:4]:
        copy.wait()
    pl.semaphore_wait(barrier, parts + groups - 2)
    for i in range(1, parts):
        gain_copy(i, t).start()
    for h in range(PIECES):
        relay(0, h)

    def pick(j):
        level = flip(z, j)
        picked = jnp.dot(disp[...], zbuf[level], preferred_element_type=F32).astype(BF16)
        for role in range(1, groups):
            xsend[level * (groups - 1) + role - 1] = picked[role * cap : (role + 1) * cap]
        x[level * CORES + c, e] = picked[:cap]
        for role in range(1, groups - 1 if j == 1 else groups):
            row_copy(level, role, e).start()
        core_copy(j, 0).start()

    def along_copy(j):
        slot = x.at[flip(z, j) * CORES + c, around[groups - 1]]
        return remote(slot, slot, ks, kr, tp=flip(z, 1) * CORES + c)

    def pass_on(j, role):
        if j == 1 and role == groups - 1:
            along_copy(1).wait_recv()
        else:
            row_copy(flip(z, j), role, around[role]).wait_recv()
        core_copy(j, role).start()

    def level_sum(j, role):
        level, source = flip(z, j), around[role]
        total, scaled = 0.0, []
        for core in range(CORES):
            part = level * CORES + core
            values = x[part, source].astype(F32)
            square = values * values
            for lane in range(0, width, 128):
                total = total + square[:, lane : lane + 128]
            scaled.append((values * gains[part]).astype(BF16))
        left = jnp.concatenate(scaled, axis=1)
        depth = pl.ds(pl.multiple_of(level * CORES * width, CORES * 128), CORES * width)
        found = (
            total,
            jnp.dot(left, gate[depth, :], preferred_element_type=F32),
            jnp.dot(left, up[depth, :], preferred_element_type=F32),
        )
        if j:
            found = [p + ref[role] for p, ref in zip(found, (squares, acc_gate, acc_up))]
        return found

    def project(k):
        batch = BATCHES[k]
        slots = x.at[0, pl.ds(0, len(batch))]
        remote(slots, slots, fs, fr.at[k], tp=z * CORES + 1 - c).wait_recv()
        for role, j in batch:
            found = level_sum(j, role)
            if j < levels - 1:
                squares[role], acc_gate[role], acc_up[role] = found
                continue
            total, gate_part, up_part = found
            scale = lax.rsqrt(jnp.sum(total, axis=1, keepdims=True) / full + EPSILON)
            gate_part = gate_part * scale
            share = 0.5 + 0.5 * jnp.tanh(0.5 * gate_part)
            hidden[role] = (gate_part * share * (up_part * scale)).astype(BF16)

    def descend(j, kind):
        level = flip(z, j)
        span = slice(groups - 1, groups) if kind else slice(0, groups - 1)
        count = 1 if kind else groups - 1
        left = hidden[span].reshape(count * cap, hidden.shape[2])

        def block(core):
            columns = pl.ds(pl.multiple_of((level * CORES + core) * width, 128), width)
            return jnp.dot(left, down[:, columns], preferred_element_type=F32)

        other, this = block(1 - c), block(c)
        half[level, span] = other.reshape(count, cap, width).astype(BF16)
        own[level, span] = this.reshape(count, cap, width)
        half_copy(level, kind).start()

    def finish(j, kind):
        level = flip(z, j)
        half_copy(level, kind).wait_recv()

        def found(role):
            rows_found = own[level, role] + half_in[level, role].astype(F32)
            if j == 0:
                rows_found = rows_found + hand_in[role].astype(F32)
            return rows_found.astype(BF16)

        if j == 0:
            hand_copy(kind).wait_recv()
        for role in (groups - 1,) if kind else range(1, groups - 1):
            if j == 1:
                hand[role] = found(role)
            else:
                back[level, role - 1] = found(role)
                back_copy(level, role).start()
        if j == 1 and kind == 0:
            hand_copy(0).start()
        if kind == 0 and j == 1:
            hand[0] = found(0)
        elif kind == 0 and j > 1:
            ret[level, 0] = found(0)
        elif kind == 0:
            return found

    def arrive(j, *roles):
        for role in roles:
            back_copy(flip(z, j), role).wait_recv()

    def settle(j):
        level = flip(z, j)
        combined = jnp.dot(
            mix[...], ret[level].reshape(groups * cap, width), preferred_element_type=F32
        )
        found = []
        for h in range(HALVES):
            part = combined[h * (rows // HALVES) : (h + 1) * (rows // HALVES)]
            for source in {3: (), 2: (3,), 0: (2,)}[j]:
                sum_copy(source, h).wait_recv()
                arrived = zin[source, h * (rows // HALVES) : (h + 1) * (rows // HALVES)]
                part = part + arrived.astype(F32)
            if j:
                zsend[j, h * (rows // HALVES) : (h + 1) * (rows // HALVES)] = part.astype(BF16)
                sum_copy(j, h).start()
            found.append(part)
        return jnp.concatenate(found, axis=0)

    spread = plan_rows()
    pick(0)
    plan_mix(spread)
    for h in range(PIECES):
        relay(1, h)
    pick(1)
    spare = gains.at[pl.ds(0, parts - 1)]
    remote(spare, spare, gs, gr, tp=flip(t, 1)).wait_recv()
    inputs[4].wait()
    loads[0].wait()
    loads[1].wait()
    relay(2, 0)
    pass_on(0, 1)
    pass_on(0, 2)
    relay(2, 1)
    project(0)
    relay(2, 2)
    relay(2, 3)
    pick(2)
    pass_on(0, 3)
    relay(3, 0)
    project(1)
    relay(3, 1)
    relay(3, 2)
    relay(3, 3)
    along_copy(0).start()
    pick(3)
    pass_on(1, 1)
    pass_on(1, 2)
    project(2)
    project(3)
    project(4)
    pass_on(1, 3)
    pass_on(2, 1)
    pass_on(2, 2)
    pass_on(2, 3)
    project(5)
    pass_on(3, 1)
    project(6)
    pass_on(3, 2)
    project(7)
    project(8)
    pass_on(3, 3)
    loads[2].wait()
    descend(3, 0)
    project(9)
    descend(3, 1)
    finish(3, 0)
    descend(1, 0)
    finish(3, 1)
    descend(1, 1)
    descend(2, 0)
    finish(1, 0)
    descend(2, 1)
    finish(1, 1)
    hand_copy(1).start()
    descend(0, 0)
    descend(0, 1)
    arrive(3, 1, 2)
    finish(2, 0)
    finish(2, 1)
    arrive(3, 3)
    settle(3)
    rest = finish(0, 0)
    arrive(2, 1, 2, 3)
    finish(0, 1)
    settle(2)
    hand_copy(2).start()
    hand_copy(2).wait_recv()
    ret[z, 0] = rest(0)
    arrive(0, 1, 2, 3)
    combined = settle(0)

    square = combined * combined
    folded = square[:, 0:128]
    for lane in range(128, width, 128):
        folded = folded + square[:, lane : lane + 128]
    stats[t] = jnp.sum(folded.T, axis=0, keepdims=True)
    for i in range(1, parts):
        stat_copy(i, t).start()
    def sent(ref, sem):
        remote(ref, ref, sem, sem, tp=flip(t, 1)).wait_send()

    for k in range(levels):

        @pl.when((z == k) & (z < levels - 1))
        def _():
            sent(zbuf.at[pl.ds(0, k + 1)], zs.at[1])

        @pl.when((z == k) & (z > 0))
        def _():
            sent(zbuf.at[pl.ds(0, levels - k)], zs.at[0])

    for ref, sem in (
        (xsend.at[pl.ds(0, levels * (groups - 1) - 1)], ns), (x.at[0, 0], ks),
        (x.at[pl.ds(0, levels)], fs), (half, ds), (hand, hs),
        (back.at[pl.ds(1, levels - 1)], qs), (zsend.at[pl.ds(2, levels - 2)], ts), (spare, gs),
    ):
        sent(ref, sem)
    seen = stats.at[pl.ds(0, parts - 1)]
    remote(seen, seen, ps, pr, tp=flip(t, 1)).wait_recv()
    total = jnp.sum(stats[...], axis=0)
    high = total.astype(BF16)
    ones = jnp.ones((1, 128), BF16)
    column = sum(
        lax.dot_general(v, ones, (((0,), (0,)), ((), ())), preferred_element_type=F32)
        for v in (high, (total - high.astype(F32)).astype(BF16))
    )
    scale = lax.rsqrt(column[:, 0:1] / full + EPSILON)
    out[...] = (combined * scale * post[...]).astype(BF16)
    sent(seen, ps)


def local_fused(tokens, pre_gain, expert_gate, expert_up, expert_down, routes, route_weights, post_gain):
    groups, parts = lax.axis_size("ep"), lax.axis_size("tp")
    rows, width = tokens.shape
    _, features, units = expert_gate.shape
    levels = parts // CORES
    cap = 3 * rows // groups
    vmem = pl.BlockSpec(memory_space=pltpu.VMEM)
    anywhere = pl.BlockSpec(memory_space=pl.ANY)
    dma = pltpu.SemaphoreType.DMA
    tok_block = pltpu.VMEM((levels, rows, width), BF16)
    block = (levels, groups, cap, width)
    away = pltpu.VMEM((levels, groups - 1, cap, width), BF16)
    return pl.pallas_call(
        functools.partial(fused, groups, parts),
        out_shape=pltpu.VMEM((rows, width), BF16),
        in_specs=[anywhere] * 8,
        out_specs=vmem,
        scratch_shapes=[
            tok_block,
            pltpu.VMEM((parts, 1, width), F32),
            pltpu.VMEM((2, rows), jnp.int32),
            pltpu.VMEM((2, rows), F32),
            pltpu.VMEM((1, width), F32),
            pltpu.VMEM((groups * cap, rows), BF16),
            pltpu.VMEM((rows, groups * cap), BF16),
            pltpu.VMEM((parts, groups, cap, width), BF16),
            pltpu.VMEM((levels * (groups - 1), cap, width), BF16),
            pltpu.VMEM((groups, cap, 128), F32),
            pltpu.VMEM((features, units), BF16),
            pltpu.VMEM((features, units), BF16),
            pltpu.VMEM((units, features), BF16),
            pltpu.VMEM((groups, cap, units), F32),
            pltpu.VMEM((groups, cap, units), F32),
            pltpu.VMEM((groups, cap, units), BF16),
            pltpu.VMEM(block, BF16),
            pltpu.VMEM(block, BF16),
            pltpu.VMEM(block, F32),
            away,
            pltpu.VMEM(block, BF16),
            pltpu.VMEM((groups, cap, width), BF16),
            pltpu.VMEM((groups, cap, width), BF16),
            tok_block,
            tok_block,
            pltpu.VMEM((parts, 1, rows), F32),
            dma((5,)), dma((3,)),
            dma((2,)), dma((levels, PIECES)),
            dma, dma,
            dma, dma((levels, groups - 1)),
            dma, dma,
            dma, dma((len(BATCHES),)),
            dma, dma((levels, 2)),
            dma, dma((levels, groups - 1)),
            dma, dma((3,)),
            dma, dma((2, HALVES)),
            dma, dma,
        ],
        compiler_params=pltpu.CompilerParams(
            collective_id=0, has_side_effects=True, vmem_limit_bytes=60 * 1024 * 1024
        ),
    )(
        tokens, pre_gain.reshape(1, width), routes.T, route_weights.T,
        expert_gate, expert_up, expert_down, post_gain.reshape(1, width),
    )


def plan(mesh):
    def choose(*args):
        tokens, gate = args[0], args[2]
        groups, parts = mesh.shape["ep"], mesh.shape["tp"]
        rows, width = tokens.shape
        fits = (
            gate.shape[0] == 1
            and groups == 4
            and parts == 4 * CORES
            and width % 128 == 0
            and rows % 128 == 0
            and (3 * rows // groups) % 64 == 0
            and gate.shape[2] % 128 == 0
        )
        return (local_fused if fits else local)(*args)

    return choose


def solution(mesh):
    placed = (
        P("ep", "tp"),
        P("tp"),
        P("ep", None, "tp"),
        P("ep", None, "tp"),
        P("ep", "tp", None),
        P("ep", None),
        P("ep", None),
        P("tp"),
    )
    return jax.shard_map(
        plan(mesh), mesh=mesh, in_specs=placed, out_specs=P("ep", "tp"), check_vma=False
    )
```

```python
import functools

import jax
import jax.numpy as jnp
from jax import lax
from jax.experimental import pallas as pl
from jax.experimental.pallas import tpu as pltpu
from jax.sharding import PartitionSpec as P

EPSILON = 1e-06


def local(tokens, pre_gain, expert_gate, expert_up, expert_down, routes, route_weights, post_gain):
    local_experts = expert_gate.shape[0]
    groups = lax.axis_size("ep")
    experts_all = local_experts * groups
    tok_rows, part_width = tokens.shape
    full_width = part_width * lax.axis_size("tp")
    capacity = 3 * tok_rows // experts_all
    values = tokens.astype(jnp.float32)
    input_sq = lax.psum(jnp.sum(values * values, axis=-1), "tp")
    normed = (
        values * lax.rsqrt(input_sq / full_width + EPSILON)[:, None] * pre_gain[None, :]
    ).astype(jnp.bfloat16)
    onehot = (routes[:, :, None] == jnp.arange(experts_all, dtype=jnp.int32)).astype(jnp.int32)
    onehot = onehot.reshape(tok_rows * 2, experts_all)
    earlier = jnp.cumsum(onehot, axis=0) - onehot
    slots = jnp.sum(earlier * onehot, axis=-1).reshape(tok_rows, 2)
    positions = routes * capacity + slots
    places = jnp.arange(experts_all * capacity, dtype=jnp.int32)
    first_pick = (places[:, None] == positions[None, :, 0]).astype(jnp.bfloat16)
    second_pick = (places[:, None] == positions[None, :, 1]).astype(jnp.bfloat16)
    dispatch = first_pick + second_pick
    outgoing = jnp.dot(dispatch, normed, preferred_element_type=jnp.float32).astype(jnp.bfloat16)
    arrived = lax.all_to_all(outgoing, "ep", split_axis=0, concat_axis=0, tiled=True)
    fragment = lax.all_gather(arrived, "tp", axis=1, tiled=True)
    count = fragment.shape[1]
    grouped = fragment.reshape(groups, local_experts, capacity, count)
    gate_pre = jnp.einsum(
        "secw,ewf->secf", grouped, expert_gate, preferred_element_type=jnp.float32
    )
    up_pre = jnp.einsum("secw,ewf->secf", grouped, expert_up, preferred_element_type=jnp.float32)
    hidden = (jax.nn.silu(gate_pre) * up_pre).astype(jnp.bfloat16)
    product = jnp.einsum("secf,efd->dsec", hidden, expert_down, preferred_element_type=jnp.float32)
    summed = lax.psum_scatter(
        product.reshape(lax.axis_size("tp") * part_width, groups * local_experts * capacity).astype(
            jnp.bfloat16
        ),
        "tp",
        scatter_dimension=0,
        tiled=True,
    )
    returned = lax.all_to_all(summed, "ep", split_axis=1, concat_axis=1, tiled=True)
    contract = (((0,), (1,)), ((), ()))
    first_out = lax.dot_general(first_pick, returned, contract, preferred_element_type=jnp.float32)
    second_out = lax.dot_general(
        second_pick, returned, contract, preferred_element_type=jnp.float32
    )
    combined = route_weights[:, 0:1] * first_out + route_weights[:, 1:2] * second_out
    output_sq = lax.psum(jnp.sum(combined * combined, axis=-1), "tp")
    scaled = combined * lax.rsqrt(output_sq / full_width + EPSILON)[:, None] * post_gain[None, :]
    return scaled.astype(jnp.bfloat16)


CORES = 2
PIECES = 4
HALVES = 4
F32 = jnp.float32
BF16 = jnp.bfloat16
MESH = pl.DeviceIdType.MESH


def flip(index, bits):
    place = 1
    while place <= bits:
        if bits & place:
            index = index + place - 2 * place * lax.rem(lax.div(index, place), 2)
        place *= 2
    return index


BATCHES = (
    ((0, 0), (0, 1)), ((1, 0), (2, 0)), ((3, 0), (0, 2)), ((1, 1), (2, 1)), ((0, 3),),
    ((1, 2), (2, 2)), ((3, 1), (3, 2)), ((1, 3),), ((2, 3),), ((3, 3),),
)


def fused(
    groups, parts, tok, gain, route_in, weight_in, gate_hbm, up_hbm, down_hbm, post_in, out,
    zbuf, gains, route, weight, post, disp, mix, x, xsend, squares,
    gate, up, down, acc_gate, acc_up, hidden, half, half_in, own, back, ret,
    hand, hand_in, zsend, zin, stats,
    isem, wsem, zs, zr, gs, gr, ns, nr, ks, kr, fs, fr, ds, dr, qs, qr, hs, hr, ts, tr, ps, pr,
):
    t, e = lax.axis_index("tp"), lax.axis_index("ep")
    z, c = lax.div(t, CORES), lax.rem(t, CORES)
    levels = parts // CORES
    rows, width = zbuf.shape[1:]
    cap = xsend.shape[1]
    full = parts * width
    around = [flip(e, role) if role else e for role in range(groups)]
    batch_of = {unit: k for k, batch in enumerate(BATCHES) for unit in batch}

    barrier = pltpu.get_barrier_semaphore()
    for i in range(1, parts):
        pl.semaphore_signal(barrier, inc=1, device_id={"tp": flip(t, i)}, device_id_type=MESH)
    for d in range(1, groups):
        pl.semaphore_signal(barrier, inc=1, device_id={"ep": flip(e, d)}, device_id_type=MESH)

    inputs = [
        pltpu.make_async_copy(route_in, route, isem.at[0]),
        pltpu.make_async_copy(weight_in, weight, isem.at[1]),
        pltpu.make_async_copy(tok, zbuf.at[z], isem.at[2]),
        pltpu.make_async_copy(gain, gains.at[t], isem.at[3]),
        pltpu.make_async_copy(post_in, post, isem.at[4]),
    ]
    for copy in inputs:
        copy.start()
    loads = [
        pltpu.make_async_copy(gate_hbm.at[0], gate, wsem.at[0]),
        pltpu.make_async_copy(up_hbm.at[0], up, wsem.at[1]),
        pltpu.make_async_copy(down_hbm.at[0], down, wsem.at[2]),
    ]
    for load in loads:
        load.start()

    def remote(src, dst, send, recv, **device):
        return pltpu.make_async_remote_copy(
            src_ref=src, dst_ref=dst, send_sem=send, recv_sem=recv,
            device_id=device, device_id_type=MESH,
        )

    def piece_of(ref, level, h, count):
        return ref.at[level, pl.ds(h * (rows // count), rows // count)]

    def token_copy(level, h, up):
        step = 1 if up else -1
        source = piece_of(zbuf, level, h, PIECES)
        return remote(source, source, zs.at[int(up)], zr.at[level, h], tp=t + step * CORES)

    def relay(k, h):
        @pl.when(z >= k)
        def _():
            if k:
                token_copy(z - k, h, True).wait_recv()

            @pl.when(z < levels - 1)
            def _():
                token_copy(z - k, h, True).start()

        @pl.when(z + k < levels)
        def _():
            if k:
                token_copy(z + k, h, False).wait_recv()

            @pl.when(z > 0)
            def _():
                token_copy(z + k, h, False).start()

    def gain_copy(i, part):
        return remote(gains.at[part], gains.at[part], gs, gr, tp=flip(t, i))

    def row_copy(level, role, source):
        return remote(
            xsend.at[level * (groups - 1) + role - 1], x.at[level * CORES + c, source],
            ns, nr.at[level, role - 1], ep=around[role],
        )

    def core_copy(j, role):
        slot = x.at[flip(z, j) * CORES + c, around[role]]
        return remote(slot, slot, fs, fr.at[batch_of[role, j]], tp=z * CORES + 1 - c)

    def half_copy(level, kind):
        span = pl.ds(groups - 1, 1) if kind else pl.ds(0, groups - 1)
        return remote(
            half.at[level, span], half_in.at[level, span],
            ds, dr.at[level, kind], tp=z * CORES + 1 - c,
        )

    def back_copy(level, role):
        return remote(
            back.at[level, role - 1], ret.at[level, role],
            qs, qr.at[level, role - 1], ep=around[role],
        )

    def hand_copy(k):
        span = (pl.ds(1, groups - 2), pl.ds(groups - 1, 1), pl.ds(0, 1))[k]
        return remote(
            hand.at[span], hand_in.at[span], hs, hr.at[k], tp=flip(z, 1) * CORES + c
        )

    def sum_copy(j, h):
        bits = 2 if j == 2 else 1
        return remote(
            piece_of(zsend, j, h, HALVES), piece_of(zin, j, h, HALVES),
            ts, tr.at[j - 2, h], tp=flip(z, bits) * CORES + c,
        )

    def stat_copy(i, part):
        return remote(stats.at[t], stats.at[part], ps, pr, tp=flip(t, i))

    def plan_rows():
        r, w = route[...], weight[...]
        first, second = r[0:1], r[1:2]
        lanes = lax.broadcasted_iota(jnp.int32, (8, rows), 0)
        names = jnp.full((8, rows), -1, jnp.int32)
        for role in range(groups):
            names = jnp.where(lanes == role, around[role], names)
        member = jnp.where((names == first) | (names == second), 1.0, 0.0)
        before = jnp.where(
            lax.broadcasted_iota(jnp.int32, (rows, rows), 0)
            < lax.broadcasted_iota(jnp.int32, (rows, rows), 1),
            1.0, 0.0,
        )
        slots = jnp.dot(member.astype(BF16), before.astype(BF16), preferred_element_type=F32)
        slots = jnp.where(member > 0.5, slots, -1.0).astype(jnp.int32)
        lines = lax.broadcasted_iota(jnp.int32, (cap, rows), 0)
        spread = []
        for role in range(groups):
            hit = lines == slots[role : role + 1]
            disp[role * cap : (role + 1) * cap, :] = jnp.where(hit, 1.0, 0.0).astype(BF16)
            chosen = jnp.where(first == around[role], w[0:1], w[1:2])
            spread.append(jnp.where(hit, chosen, 0.0))
        return spread

    def plan_mix(spread):
        mix[...] = jnp.concatenate(spread, axis=0).T.astype(BF16)

    for copy in inputs[:4]:
        copy.wait()
    pl.semaphore_wait(barrier, parts + groups - 2)
    for i in range(1, parts):
        gain_copy(i, t).start()
    for h in range(PIECES):
        relay(0, h)

    def pick(j):
        level = flip(z, j)
        picked = jnp.dot(disp[...], zbuf[level], preferred_element_type=F32).astype(BF16)
        for role in range(1, groups):
            xsend[level * (groups - 1) + role - 1] = picked[role * cap : (role + 1) * cap]
        x[level * CORES + c, e] = picked[:cap]
        for role in range(1, groups - 1 if j == 1 else groups):
            row_copy(level, role, e).start()
        core_copy(j, 0).start()

    def along_copy(j):
        slot = x.at[flip(z, j) * CORES + c, around[groups - 1]]
        return remote(slot, slot, ks, kr, tp=flip(z, 1) * CORES + c)

    def pass_on(j, role):
        if j == 1 and role == groups - 1:
            along_copy(1).wait_recv()
        else:
            row_copy(flip(z, j), role, around[role]).wait_recv()
        core_copy(j, role).start()

    def level_sum(j, role):
        level, source = flip(z, j), around[role]
        total, scaled = 0.0, []
        for core in range(CORES):
            part = level * CORES + core
            values = x[part, source].astype(F32)
            square = values * values
            for lane in range(0, width, 128):
                total = total + square[:, lane : lane + 128]
            scaled.append((values * gains[part]).astype(BF16))
        left = jnp.concatenate(scaled, axis=1)
        depth = pl.ds(pl.multiple_of(level * CORES * width, CORES * 128), CORES * width)
        found = (
            total,
            jnp.dot(left, gate[depth, :], preferred_element_type=F32),
            jnp.dot(left, up[depth, :], preferred_element_type=F32),
        )
        if j:
            found = [p + ref[role] for p, ref in zip(found, (squares, acc_gate, acc_up))]
        return found

    def project(k):
        batch = BATCHES[k]
        slots = x.at[0, pl.ds(0, len(batch))]
        remote(slots, slots, fs, fr.at[k], tp=z * CORES + 1 - c).wait_recv()
        for role, j in batch:
            found = level_sum(j, role)
            if j < levels - 1:
                squares[role], acc_gate[role], acc_up[role] = found
                continue
            total, gate_part, up_part = found
            scale = lax.rsqrt(jnp.sum(total, axis=1, keepdims=True) / full + EPSILON)
            gate_part = gate_part * scale
            share = 0.5 + 0.5 * jnp.tanh(0.5 * gate_part)
            hidden[role] = (gate_part * share * (up_part * scale)).astype(BF16)

    def descend(j, kind):
        level = flip(z, j)
        span = slice(groups - 1, groups) if kind else slice(0, groups - 1)
        count = 1 if kind else groups - 1
        left = hidden[span].reshape(count * cap, hidden.shape[2])

        def block(core):
            columns = pl.ds(pl.multiple_of((level * CORES + core) * width, 128), width)
            return jnp.dot(left, down[:, columns], preferred_element_type=F32)

        other, this = block(1 - c), block(c)
        half[level, span] = other.reshape(count, cap, width).astype(BF16)
        own[level, span] = this.reshape(count, cap, width)
        half_copy(level, kind).start()

    def finish(j, kind):
        level = flip(z, j)
        half_copy(level, kind).wait_recv()

        def found(role):
            rows_found = own[level, role] + half_in[level, role].astype(F32)
            if j == 0:
                rows_found = rows_found + hand_in[role].astype(F32)
            return rows_found.astype(BF16)

        if j == 0:
            hand_copy(kind).wait_recv()
        for role in (groups - 1,) if kind else range(1, groups - 1):
            if j == 1:
                hand[role] = found(role)
            else:
                back[level, role - 1] = found(role)
                back_copy(level, role).start()
        if j == 1 and kind == 0:
            hand_copy(0).start()
        if kind == 0 and j == 1:
            hand[0] = found(0)
        elif kind == 0 and j > 1:
            ret[level, 0] = found(0)
        elif kind == 0:
            return found

    def arrive(j, *roles):
        for role in roles:
            back_copy(flip(z, j), role).wait_recv()

    def settle(j):
        level = flip(z, j)
        combined = jnp.dot(
            mix[...], ret[level].reshape(groups * cap, width), preferred_element_type=F32
        )
        found = []
        for h in range(HALVES):
            part = combined[h * (rows // HALVES) : (h + 1) * (rows // HALVES)]
            for source in {3: (), 2: (3,), 0: (2,)}[j]:
                sum_copy(source, h).wait_recv()
                arrived = zin[source, h * (rows // HALVES) : (h + 1) * (rows // HALVES)]
                part = part + arrived.astype(F32)
            if j:
                zsend[j, h * (rows // HALVES) : (h + 1) * (rows // HALVES)] = part.astype(BF16)
                sum_copy(j, h).start()
            found.append(part)
        return jnp.concatenate(found, axis=0)

    spread = plan_rows()
    pick(0)
    plan_mix(spread)
    for h in range(PIECES):
        relay(1, h)
    pick(1)
    spare = gains.at[pl.ds(0, parts - 1)]
    remote(spare, spare, gs, gr, tp=flip(t, 1)).wait_recv()
    inputs[4].wait()
    loads[0].wait()
    loads[1].wait()
    relay(2, 0)
    pass_on(0, 1)
    pass_on(0, 2)
    relay(2, 1)
    relay(2, 2)
    relay(2, 3)
    pick(2)
    project(0)
    pass_on(0, 3)
    relay(3, 0)
    project(1)
    relay(3, 1)
    relay(3, 2)
    relay(3, 3)
    along_copy(0).start()
    pick(3)
    pass_on(1, 1)
    pass_on(1, 2)
    project(2)
    project(3)
    project(4)
    pass_on(1, 3)
    pass_on(2, 1)
    pass_on(2, 2)
    pass_on(2, 3)
    project(5)
    pass_on(3, 1)
    project(6)
    pass_on(3, 2)
    project(7)
    project(8)
    pass_on(3, 3)
    loads[2].wait()
    descend(3, 0)
    descend(1, 0)
    project(9)
    finish(3, 0)
    descend(3, 1)
    descend(1, 1)
    finish(1, 0)
    descend(2, 0)
    finish(3, 1)
    descend(2, 1)
    finish(1, 1)
    hand_copy(1).start()
    descend(0, 0)
    descend(0, 1)
    finish(2, 0)
    finish(2, 1)
    arrive(3, 1, 2, 3)
    settle(3)
    rest = finish(0, 0)
    finish(0, 1)
    arrive(2, 1, 2, 3)
    settle(2)
    hand_copy(2).start()
    hand_copy(2).wait_recv()
    ret[z, 0] = rest(0)
    arrive(0, 1, 2, 3)
    combined = settle(0)

    square = combined * combined
    folded = square[:, 0:128]
    for lane in range(128, width, 128):
        folded = folded + square[:, lane : lane + 128]
    stats[t] = jnp.sum(folded.T, axis=0, keepdims=True)
    for i in range(1, parts):
        stat_copy(i, t).start()
    def sent(ref, sem):
        remote(ref, ref, sem, sem, tp=flip(t, 1)).wait_send()

    for k in range(levels):

        @pl.when((z == k) & (z < levels - 1))
        def _():
            sent(zbuf.at[pl.ds(0, k + 1)], zs.at[1])

        @pl.when((z == k) & (z > 0))
        def _():
            sent(zbuf.at[pl.ds(0, levels - k)], zs.at[0])

    for ref, sem in (
        (xsend.at[pl.ds(0, levels * (groups - 1) - 1)], ns), (x.at[0, 0], ks),
        (x.at[pl.ds(0, levels)], fs), (half, ds), (hand, hs),
        (back.at[pl.ds(1, levels - 1)], qs), (zsend.at[pl.ds(2, levels - 2)], ts), (spare, gs),
    ):
        sent(ref, sem)
    seen = stats.at[pl.ds(0, parts - 1)]
    remote(seen, seen, ps, pr, tp=flip(t, 1)).wait_recv()
    total = jnp.sum(stats[...], axis=0)
    high = total.astype(BF16)
    ones = jnp.ones((1, 128), BF16)
    column = sum(
        lax.dot_general(v, ones, (((0,), (0,)), ((), ())), preferred_element_type=F32)
        for v in (high, (total - high.astype(F32)).astype(BF16))
    )
    scale = lax.rsqrt(column[:, 0:1] / full + EPSILON)
    out[...] = (combined * scale * post[...]).astype(BF16)
    sent(seen, ps)


def local_fused(tokens, pre_gain, expert_gate, expert_up, expert_down, routes, route_weights, post_gain):
    groups, parts = lax.axis_size("ep"), lax.axis_size("tp")
    rows, width = tokens.shape
    _, features, units = expert_gate.shape
    levels = parts // CORES
    cap = 3 * rows // groups
    vmem = pl.BlockSpec(memory_space=pltpu.VMEM)
    anywhere = pl.BlockSpec(memory_space=pl.ANY)
    dma = pltpu.SemaphoreType.DMA
    tok_block = pltpu.VMEM((levels, rows, width), BF16)
    block = (levels, groups, cap, width)
    away = pltpu.VMEM((levels, groups - 1, cap, width), BF16)
    return pl.pallas_call(
        functools.partial(fused, groups, parts),
        out_shape=pltpu.VMEM((rows, width), BF16),
        in_specs=[anywhere] * 8,
        out_specs=vmem,
        scratch_shapes=[
            tok_block,
            pltpu.VMEM((parts, 1, width), F32),
            pltpu.VMEM((2, rows), jnp.int32),
            pltpu.VMEM((2, rows), F32),
            pltpu.VMEM((1, width), F32),
            pltpu.VMEM((groups * cap, rows), BF16),
            pltpu.VMEM((rows, groups * cap), BF16),
            pltpu.VMEM((parts, groups, cap, width), BF16),
            pltpu.VMEM((levels * (groups - 1), cap, width), BF16),
            pltpu.VMEM((groups, cap, 128), F32),
            pltpu.VMEM((features, units), BF16),
            pltpu.VMEM((features, units), BF16),
            pltpu.VMEM((units, features), BF16),
            pltpu.VMEM((groups, cap, units), F32),
            pltpu.VMEM((groups, cap, units), F32),
            pltpu.VMEM((groups, cap, units), BF16),
            pltpu.VMEM(block, BF16),
            pltpu.VMEM(block, BF16),
            pltpu.VMEM(block, F32),
            away,
            pltpu.VMEM(block, BF16),
            pltpu.VMEM((groups, cap, width), BF16),
            pltpu.VMEM((groups, cap, width), BF16),
            tok_block,
            tok_block,
            pltpu.VMEM((parts, 1, rows), F32),
            dma((5,)), dma((3,)),
            dma((2,)), dma((levels, PIECES)),
            dma, dma,
            dma, dma((levels, groups - 1)),
            dma, dma,
            dma, dma((len(BATCHES),)),
            dma, dma((levels, 2)),
            dma, dma((levels, groups - 1)),
            dma, dma((3,)),
            dma, dma((2, HALVES)),
            dma, dma,
        ],
        compiler_params=pltpu.CompilerParams(
            collective_id=0, has_side_effects=True, vmem_limit_bytes=60 * 1024 * 1024
        ),
    )(
        tokens, pre_gain.reshape(1, width), routes.T, route_weights.T,
        expert_gate, expert_up, expert_down, post_gain.reshape(1, width),
    )


def plan(mesh):
    def choose(*args):
        tokens, gate = args[0], args[2]
        groups, parts = mesh.shape["ep"], mesh.shape["tp"]
        rows, width = tokens.shape
        fits = (
            gate.shape[0] == 1
            and groups == 4
            and parts == 4 * CORES
            and width % 128 == 0
            and rows % 128 == 0
            and (3 * rows // groups) % 64 == 0
            and gate.shape[2] % 128 == 0
        )
        return (local_fused if fits else local)(*args)

    return choose


def solution(mesh):
    placed = (
        P("ep", "tp"),
        P("tp"),
        P("ep", None, "tp"),
        P("ep", None, "tp"),
        P("ep", "tp", None),
        P("ep", None),
        P("ep", None),
        P("tp"),
    )
    return jax.shard_map(
        plan(mesh), mesh=mesh, in_specs=placed, out_specs=P("ep", "tp"), check_vma=False
    )
```

```python
import functools

import jax
import jax.numpy as jnp
from jax import lax
from jax.experimental import pallas as pl
from jax.experimental.pallas import tpu as pltpu
from jax.sharding import PartitionSpec as P

EPSILON = 1e-06


def local(tokens, pre_gain, expert_gate, expert_up, expert_down, routes, route_weights, post_gain):
    local_experts = expert_gate.shape[0]
    groups = lax.axis_size("ep")
    experts_all = local_experts * groups
    tok_rows, part_width = tokens.shape
    full_width = part_width * lax.axis_size("tp")
    capacity = 3 * tok_rows // experts_all
    values = tokens.astype(jnp.float32)
    input_sq = lax.psum(jnp.sum(values * values, axis=-1), "tp")
    normed = (
        values * lax.rsqrt(input_sq / full_width + EPSILON)[:, None] * pre_gain[None, :]
    ).astype(jnp.bfloat16)
    onehot = (routes[:, :, None] == jnp.arange(experts_all, dtype=jnp.int32)).astype(jnp.int32)
    onehot = onehot.reshape(tok_rows * 2, experts_all)
    earlier = jnp.cumsum(onehot, axis=0) - onehot
    slots = jnp.sum(earlier * onehot, axis=-1).reshape(tok_rows, 2)
    positions = routes * capacity + slots
    places = jnp.arange(experts_all * capacity, dtype=jnp.int32)
    first_pick = (places[:, None] == positions[None, :, 0]).astype(jnp.bfloat16)
    second_pick = (places[:, None] == positions[None, :, 1]).astype(jnp.bfloat16)
    dispatch = first_pick + second_pick
    outgoing = jnp.dot(dispatch, normed, preferred_element_type=jnp.float32).astype(jnp.bfloat16)
    arrived = lax.all_to_all(outgoing, "ep", split_axis=0, concat_axis=0, tiled=True)
    fragment = lax.all_gather(arrived, "tp", axis=1, tiled=True)
    count = fragment.shape[1]
    grouped = fragment.reshape(groups, local_experts, capacity, count)
    gate_pre = jnp.einsum(
        "secw,ewf->secf", grouped, expert_gate, preferred_element_type=jnp.float32
    )
    up_pre = jnp.einsum("secw,ewf->secf", grouped, expert_up, preferred_element_type=jnp.float32)
    hidden = (jax.nn.silu(gate_pre) * up_pre).astype(jnp.bfloat16)
    product = jnp.einsum("secf,efd->dsec", hidden, expert_down, preferred_element_type=jnp.float32)
    summed = lax.psum_scatter(
        product.reshape(lax.axis_size("tp") * part_width, groups * local_experts * capacity).astype(
            jnp.bfloat16
        ),
        "tp",
        scatter_dimension=0,
        tiled=True,
    )
    returned = lax.all_to_all(summed, "ep", split_axis=1, concat_axis=1, tiled=True)
    contract = (((0,), (1,)), ((), ()))
    first_out = lax.dot_general(first_pick, returned, contract, preferred_element_type=jnp.float32)
    second_out = lax.dot_general(
        second_pick, returned, contract, preferred_element_type=jnp.float32
    )
    combined = route_weights[:, 0:1] * first_out + route_weights[:, 1:2] * second_out
    output_sq = lax.psum(jnp.sum(combined * combined, axis=-1), "tp")
    scaled = combined * lax.rsqrt(output_sq / full_width + EPSILON)[:, None] * post_gain[None, :]
    return scaled.astype(jnp.bfloat16)


CORES = 2
PIECES = 4
HALVES = 2
F32 = jnp.float32
BF16 = jnp.bfloat16
MESH = pl.DeviceIdType.MESH


def flip(index, bits):
    place = 1
    while place <= bits:
        if bits & place:
            index = index + place - 2 * place * lax.rem(lax.div(index, place), 2)
        place *= 2
    return index


BATCHES = (
    ((0, 0), (0, 1)), ((1, 0), (2, 0)), ((3, 0), (0, 2)), ((1, 1), (2, 1)), ((0, 3),),
    ((1, 2), (2, 2)), ((3, 1), (3, 2)), ((1, 3),), ((2, 3),), ((3, 3),),
)


def fused(
    groups, parts, tok, gain, route_in, weight_in, gate_hbm, up_hbm, down_hbm, post_in, out,
    zbuf, gains, route, weight, post, disp, mix, x, xsend, squares,
    gate, up, down, acc_gate, acc_up, hidden, half, half_in, own, back, ret,
    hand, hand_in, zsend, zin, stats,
    isem, wsem, zs, zr, gs, gr, ns, nr, ks, kr, fs, fr, ds, dr, qs, qr, hs, hr, ts, tr, ps, pr,
):
    t, e = lax.axis_index("tp"), lax.axis_index("ep")
    z, c = lax.div(t, CORES), lax.rem(t, CORES)
    levels = parts // CORES
    rows, width = zbuf.shape[1:]
    cap = xsend.shape[1]
    full = parts * width
    around = [flip(e, role) if role else e for role in range(groups)]
    batch_of = {unit: k for k, batch in enumerate(BATCHES) for unit in batch}

    barrier = pltpu.get_barrier_semaphore()
    for i in range(1, parts):
        pl.semaphore_signal(barrier, inc=1, device_id={"tp": flip(t, i)}, device_id_type=MESH)
    for d in range(1, groups):
        pl.semaphore_signal(barrier, inc=1, device_id={"ep": flip(e, d)}, device_id_type=MESH)

    inputs = [
        pltpu.make_async_copy(route_in, route, isem.at[0]),
        pltpu.make_async_copy(weight_in, weight, isem.at[1]),
        pltpu.make_async_copy(tok, zbuf.at[z], isem.at[2]),
        pltpu.make_async_copy(gain, gains.at[t], isem.at[3]),
        pltpu.make_async_copy(post_in, post, isem.at[4]),
    ]
    for copy in inputs:
        copy.start()
    loads = [
        pltpu.make_async_copy(gate_hbm.at[0], gate, wsem.at[0]),
        pltpu.make_async_copy(up_hbm.at[0], up, wsem.at[1]),
        pltpu.make_async_copy(down_hbm.at[0], down, wsem.at[2]),
    ]
    for load in loads:
        load.start()

    def remote(src, dst, send, recv, **device):
        return pltpu.make_async_remote_copy(
            src_ref=src, dst_ref=dst, send_sem=send, recv_sem=recv,
            device_id=device, device_id_type=MESH,
        )

    def piece_of(ref, level, h, count):
        return ref.at[level, pl.ds(h * (rows // count), rows // count)]

    def token_copy(level, h, up):
        step = 1 if up else -1
        source = piece_of(zbuf, level, h, PIECES)
        return remote(source, source, zs.at[int(up)], zr.at[level, h], tp=t + step * CORES)

    def relay(k, h):
        @pl.when(z >= k)
        def _():
            if k:
                token_copy(z - k, h, True).wait_recv()

            @pl.when(z < levels - 1)
            def _():
                token_copy(z - k, h, True).start()

        @pl.when(z + k < levels)
        def _():
            if k:
                token_copy(z + k, h, False).wait_recv()

            @pl.when(z > 0)
            def _():
                token_copy(z + k, h, False).start()

    def gain_copy(i, part):
        return remote(gains.at[part], gains.at[part], gs, gr, tp=flip(t, i))

    def row_copy(level, role, source):
        return remote(
            xsend.at[level * (groups - 1) + role - 1], x.at[level * CORES + c, source],
            ns, nr.at[level, role - 1], ep=around[role],
        )

    def core_copy(j, role):
        slot = x.at[flip(z, j) * CORES + c, around[role]]
        return remote(slot, slot, fs, fr.at[batch_of[role, j]], tp=z * CORES + 1 - c)

    def half_copy(level, kind):
        span = pl.ds(groups - 1, 1) if kind else pl.ds(0, groups - 1)
        return remote(
            half.at[level, span], half_in.at[level, span],
            ds, dr.at[level, kind], tp=z * CORES + 1 - c,
        )

    def back_copy(level, role):
        return remote(
            back.at[level, role - 1], ret.at[level, role],
            qs, qr.at[level], ep=around[role],
        )

    def hand_copy(k):
        span = (pl.ds(1, groups - 2), pl.ds(groups - 1, 1), pl.ds(0, 1))[k]
        return remote(
            hand.at[span], hand_in.at[span], hs, hr.at[k], tp=flip(z, 1) * CORES + c
        )

    def sum_copy(j, h):
        bits = 2 if j == 2 else 1
        return remote(
            piece_of(zsend, j, h, HALVES), piece_of(zin, j, h, HALVES),
            ts, tr.at[j - 2, h], tp=flip(z, bits) * CORES + c,
        )

    def stat_copy(i, part):
        return remote(stats.at[t], stats.at[part], ps, pr, tp=flip(t, i))

    def plan_rows():
        r, w = route[...], weight[...]
        first, second = r[0:1], r[1:2]
        lanes = lax.broadcasted_iota(jnp.int32, (8, rows), 0)
        names = jnp.full((8, rows), -1, jnp.int32)
        for role in range(groups):
            names = jnp.where(lanes == role, around[role], names)
        member = jnp.where((names == first) | (names == second), 1.0, 0.0)
        before = jnp.where(
            lax.broadcasted_iota(jnp.int32, (rows, rows), 0)
            < lax.broadcasted_iota(jnp.int32, (rows, rows), 1),
            1.0, 0.0,
        )
        slots = jnp.dot(member.astype(BF16), before.astype(BF16), preferred_element_type=F32)
        slots = jnp.where(member > 0.5, slots, -1.0).astype(jnp.int32)
        lines = lax.broadcasted_iota(jnp.int32, (cap, rows), 0)
        spread = []
        for role in range(groups):
            hit = lines == slots[role : role + 1]
            disp[role * cap : (role + 1) * cap, :] = jnp.where(hit, 1.0, 0.0).astype(BF16)
            chosen = jnp.where(first == around[role], w[0:1], w[1:2])
            spread.append(jnp.where(hit, chosen, 0.0))
        return spread

    def plan_mix(spread):
        mix[...] = jnp.concatenate(spread, axis=0).T.astype(BF16)

    for copy in inputs[:4]:
        copy.wait()
    pl.semaphore_wait(barrier, parts + groups - 2)
    for i in range(1, parts):
        gain_copy(i, t).start()
    for h in range(PIECES):
        relay(0, h)

    def pick(j):
        level = flip(z, j)
        picked = jnp.dot(disp[...], zbuf[level], preferred_element_type=F32).astype(BF16)
        for role in range(1, groups):
            xsend[level * (groups - 1) + role - 1] = picked[role * cap : (role + 1) * cap]
        x[level * CORES + c, e] = picked[:cap]
        for role in range(1, groups - 1 if j == 1 else groups):
            row_copy(level, role, e).start()
        core_copy(j, 0).start()

    def along_copy(j):
        slot = x.at[flip(z, j) * CORES + c, around[groups - 1]]
        return remote(slot, slot, ks, kr, tp=flip(z, 1) * CORES + c)

    def pass_on(j, role):
        if j == 1 and role == groups - 1:
            along_copy(1).wait_recv()
        else:
            row_copy(flip(z, j), role, around[role]).wait_recv()
        core_copy(j, role).start()

    def level_sum(j, role):
        level, source = flip(z, j), around[role]
        total, scaled = 0.0, []
        for core in range(CORES):
            part = level * CORES + core
            values = x[part, source].astype(F32)
            square = values * values
            for lane in range(0, width, 128):
                total = total + square[:, lane : lane + 128]
            scaled.append((values * gains[part]).astype(BF16))
        left = jnp.concatenate(scaled, axis=1)
        depth = pl.ds(pl.multiple_of(level * CORES * width, CORES * 128), CORES * width)
        found = (
            total,
            jnp.dot(left, gate[depth, :], preferred_element_type=F32),
            jnp.dot(left, up[depth, :], preferred_element_type=F32),
        )
        if j:
            found = [p + ref[role] for p, ref in zip(found, (squares, acc_gate, acc_up))]
        return found

    def project(k):
        batch = BATCHES[k]
        slots = x.at[0, pl.ds(0, len(batch))]
        remote(slots, slots, fs, fr.at[k], tp=z * CORES + 1 - c).wait_recv()
        for role, j in batch:
            found = level_sum(j, role)
            if j < levels - 1:
                squares[role], acc_gate[role], acc_up[role] = found
                continue
            total, gate_part, up_part = found
            scale = lax.rsqrt(jnp.sum(total, axis=1, keepdims=True) / full + EPSILON)
            gate_part = gate_part * scale
            share = 0.5 + 0.5 * jnp.tanh(0.5 * gate_part)
            hidden[role] = (gate_part * share * (up_part * scale)).astype(BF16)

    def descend(j, kind):
        level = flip(z, j)
        span = slice(groups - 1, groups) if kind else slice(0, groups - 1)
        count = 1 if kind else groups - 1
        left = hidden[span].reshape(count * cap, hidden.shape[2])

        def block(core):
            columns = pl.ds(pl.multiple_of((level * CORES + core) * width, 128), width)
            return jnp.dot(left, down[:, columns], preferred_element_type=F32)

        other, this = block(1 - c), block(c)
        half[level, span] = other.reshape(count, cap, width).astype(BF16)
        own[level, span] = this.reshape(count, cap, width)
        half_copy(level, kind).start()

    def finish(j, kind):
        level = flip(z, j)
        half_copy(level, kind).wait_recv()

        def found(role):
            rows_found = own[level, role] + half_in[level, role].astype(F32)
            if j == 0:
                rows_found = rows_found + hand_in[role].astype(F32)
            return rows_found.astype(BF16)

        if j == 0:
            hand_copy(kind).wait_recv()
        for role in (groups - 1,) if kind else range(1, groups - 1):
            if j == 1:
                hand[role] = found(role)
            else:
                back[level, role - 1] = found(role)
                back_copy(level, role).start()
        if j == 1 and kind == 0:
            hand_copy(0).start()
        if kind == 0 and j == 1:
            hand[0] = found(0)
        elif kind == 0 and j > 1:
            ret[level, 0] = found(0)
        elif kind == 0:
            return found

    def arrive(j):
        level = flip(z, j)
        found = ret.at[level, pl.ds(1, groups - 1)]
        remote(found, found, qs, qr.at[level], ep=around[1]).wait_recv()

    def settle(j):
        level = flip(z, j)
        combined = jnp.dot(
            mix[...], ret[level].reshape(groups * cap, width), preferred_element_type=F32
        )
        found = []
        for h in range(HALVES):
            part = combined[h * (rows // HALVES) : (h + 1) * (rows // HALVES)]
            for source in {3: (), 2: (3,), 0: (2,)}[j]:
                sum_copy(source, h).wait_recv()
                arrived = zin[source, h * (rows // HALVES) : (h + 1) * (rows // HALVES)]
                part = part + arrived.astype(F32)
            if j:
                zsend[j, h * (rows // HALVES) : (h + 1) * (rows // HALVES)] = part.astype(BF16)
                sum_copy(j, h).start()
            found.append(part)
        return jnp.concatenate(found, axis=0)

    spread = plan_rows()
    pick(0)
    plan_mix(spread)
    for h in range(PIECES):
        relay(1, h)
    pick(1)
    spare = gains.at[pl.ds(0, parts - 1)]
    remote(spare, spare, gs, gr, tp=flip(t, 1)).wait_recv()
    inputs[4].wait()
    loads[0].wait()
    loads[1].wait()
    relay(2, 0)
    pass_on(0, 1)
    pass_on(0, 2)
    relay(2, 1)
    relay(2, 2)
    relay(2, 3)
    pick(2)
    project(0)
    pass_on(0, 3)
    relay(3, 0)
    project(1)
    relay(3, 1)
    relay(3, 2)
    relay(3, 3)
    along_copy(0).start()
    pick(3)
    pass_on(1, 1)
    pass_on(1, 2)
    project(2)
    project(3)
    project(4)
    pass_on(1, 3)
    pass_on(2, 1)
    pass_on(2, 2)
    pass_on(2, 3)
    project(5)
    pass_on(3, 1)
    project(6)
    pass_on(3, 2)
    project(7)
    project(8)
    pass_on(3, 3)
    loads[2].wait()
    descend(3, 0)
    descend(1, 0)
    project(9)
    finish(3, 0)
    descend(3, 1)
    descend(1, 1)
    finish(1, 0)
    descend(2, 0)
    finish(3, 1)
    descend(2, 1)
    finish(1, 1)
    hand_copy(1).start()
    descend(0, 0)
    descend(0, 1)
    finish(2, 0)
    finish(2, 1)
    arrive(3)
    settle(3)
    rest = finish(0, 0)
    finish(0, 1)
    arrive(2)
    settle(2)
    hand_copy(2).start()
    hand_copy(2).wait_recv()
    ret[z, 0] = rest(0)
    arrive(0)
    combined = settle(0)

    square = combined * combined
    folded = square[:, 0:128]
    for lane in range(128, width, 128):
        folded = folded + square[:, lane : lane + 128]
    stats[t] = jnp.sum(folded.T, axis=0, keepdims=True)
    for i in range(1, parts):
        stat_copy(i, t).start()
    def sent(ref, sem):
        remote(ref, ref, sem, sem, tp=flip(t, 1)).wait_send()

    for k in range(levels):

        @pl.when((z == k) & (z < levels - 1))
        def _():
            sent(zbuf.at[pl.ds(0, k + 1)], zs.at[1])

        @pl.when((z == k) & (z > 0))
        def _():
            sent(zbuf.at[pl.ds(0, levels - k)], zs.at[0])

    for ref, sem in (
        (xsend.at[pl.ds(0, levels * (groups - 1) - 1)], ns), (x.at[0, 0], ks),
        (x.at[pl.ds(0, levels)], fs), (half, ds), (hand, hs),
        (back.at[pl.ds(1, levels - 1)], qs), (zsend.at[pl.ds(2, levels - 2)], ts), (spare, gs),
    ):
        sent(ref, sem)
    seen = stats.at[pl.ds(0, parts - 1)]
    remote(seen, seen, ps, pr, tp=flip(t, 1)).wait_recv()
    total = jnp.sum(stats[...], axis=0)
    high = total.astype(BF16)
    ones = jnp.ones((1, 128), BF16)
    column = sum(
        lax.dot_general(v, ones, (((0,), (0,)), ((), ())), preferred_element_type=F32)
        for v in (high, (total - high.astype(F32)).astype(BF16))
    )
    scale = lax.rsqrt(column[:, 0:1] / full + EPSILON)
    out[...] = (combined * scale * post[...]).astype(BF16)
    sent(seen, ps)


def local_fused(tokens, pre_gain, expert_gate, expert_up, expert_down, routes, route_weights, post_gain):
    groups, parts = lax.axis_size("ep"), lax.axis_size("tp")
    rows, width = tokens.shape
    _, features, units = expert_gate.shape
    levels = parts // CORES
    cap = 3 * rows // groups
    vmem = pl.BlockSpec(memory_space=pltpu.VMEM)
    anywhere = pl.BlockSpec(memory_space=pl.ANY)
    dma = pltpu.SemaphoreType.DMA
    tok_block = pltpu.VMEM((levels, rows, width), BF16)
    block = (levels, groups, cap, width)
    away = pltpu.VMEM((levels, groups - 1, cap, width), BF16)
    return pl.pallas_call(
        functools.partial(fused, groups, parts),
        out_shape=pltpu.VMEM((rows, width), BF16),
        in_specs=[anywhere] * 8,
        out_specs=vmem,
        scratch_shapes=[
            tok_block,
            pltpu.VMEM((parts, 1, width), F32),
            pltpu.VMEM((2, rows), jnp.int32),
            pltpu.VMEM((2, rows), F32),
            pltpu.VMEM((1, width), F32),
            pltpu.VMEM((groups * cap, rows), BF16),
            pltpu.VMEM((rows, groups * cap), BF16),
            pltpu.VMEM((parts, groups, cap, width), BF16),
            pltpu.VMEM((levels * (groups - 1), cap, width), BF16),
            pltpu.VMEM((groups, cap, 128), F32),
            pltpu.VMEM((features, units), BF16),
            pltpu.VMEM((features, units), BF16),
            pltpu.VMEM((units, features), BF16),
            pltpu.VMEM((groups, cap, units), F32),
            pltpu.VMEM((groups, cap, units), F32),
            pltpu.VMEM((groups, cap, units), BF16),
            pltpu.VMEM(block, BF16),
            pltpu.VMEM(block, BF16),
            pltpu.VMEM(block, F32),
            away,
            pltpu.VMEM(block, BF16),
            pltpu.VMEM((groups, cap, width), BF16),
            pltpu.VMEM((groups, cap, width), BF16),
            tok_block,
            tok_block,
            pltpu.VMEM((parts, 1, rows), F32),
            dma((5,)), dma((3,)),
            dma((2,)), dma((levels, PIECES)),
            dma, dma,
            dma, dma((levels, groups - 1)),
            dma, dma,
            dma, dma((len(BATCHES),)),
            dma, dma((levels, 2)),
            dma, dma((levels,)),
            dma, dma((3,)),
            dma, dma((2, HALVES)),
            dma, dma,
        ],
        compiler_params=pltpu.CompilerParams(
            collective_id=0, has_side_effects=True, vmem_limit_bytes=60 * 1024 * 1024
        ),
    )(
        tokens, pre_gain.reshape(1, width), routes.T, route_weights.T,
        expert_gate, expert_up, expert_down, post_gain.reshape(1, width),
    )


def plan(mesh):
    def choose(*args):
        tokens, gate = args[0], args[2]
        groups, parts = mesh.shape["ep"], mesh.shape["tp"]
        rows, width = tokens.shape
        fits = (
            gate.shape[0] == 1
            and groups == 4
            and parts == 4 * CORES
            and width % 128 == 0
            and rows % 128 == 0
            and (3 * rows // groups) % 64 == 0
            and gate.shape[2] % 128 == 0
        )
        return (local_fused if fits else local)(*args)

    return choose


def solution(mesh):
    placed = (
        P("ep", "tp"),
        P("tp"),
        P("ep", None, "tp"),
        P("ep", None, "tp"),
        P("ep", "tp", None),
        P("ep", None),
        P("ep", None),
        P("tp"),
    )
    return jax.shard_map(
        plan(mesh), mesh=mesh, in_specs=placed, out_specs=P("ep", "tp"), check_vma=False
    )
```
